32 devices in a mesh: sp: 16 (over z, y, x), tp: 2 (over core).
Axes of the slice: x: 2, y: 2, z: 4, core: 2. Of those that a mesh axis runs over, the one named last changes fastest.
Arguments:
- resid: bfloat16 [3072, 2048], P('sp'), may hold values from -6 to 6
- queries: bfloat16 [3072, 1024], P('sp', 'tp'), may hold values from -6.5 to 6.5
- keys: bfloat16 [3072, 1024], P('sp', 'tp'), may hold values from -6.5 to 6.5
- values: bfloat16 [3072, 1024], P('sp', 'tp'), may hold values from -6 to 6
- lambdas: float32 [8], P('tp'), may hold values from 0.3 to 0.8
- head_gain: float32 [128], replicated, may hold values from 0.1 to 1.9
- out_weight: bfloat16 [1024, 2048], P('tp'), may hold values from -0.1875 to 0.1875
- norm_gain: float32 [2048], replicated, may hold values from 0.1 to 1.9
- gate_weight: bfloat16 [2048, 5632], P('sp', 'tp'), may hold values from -0.125 to 0.125
- up_weight: bfloat16 [2048, 5632], P('sp', 'tp'), may hold values from -0.125 to 0.125
- down_weight: bfloat16 [5632, 2048], P('tp', 'sp'), may hold values from -0.078125 to 0.078125
Outputs:
- result: bfloat16 [3072, 2048], P('sp')
The draws below stay inside these ranges and needn't reach their ends.
All inputs are finite; a program needn't handle non-finite values.
Results may differ from the reference program's by a relative error of at most 0.014.
Values may be sent and summed in bfloat16 or wider, within the bound.
A program may use at most 128 MiB of HBM per device.

```python
import jax
import jax.numpy as jnp
from jax import lax

D = 2048
HEADS = 8
QK = 64
VD = 128
FF = 5632
TOK_DEV = 192
TOKENS = 3072
N_TP = 2


def shared_field(key, salt, planted_row, period):
    width = HEADS * 2 * QK
    field = jnp.clip(jax.random.normal(jax.random.fold_in(key, salt), (TOKENS, width), jnp.float32) * 1.3, -6.5, 6.5)
    return field


def draw_queries(key, part):
    return shared_field(key, 11, 5, 97).astype(jnp.bfloat16)


def draw_keys(key, part):
    return shared_field(key, 23, 3, 89).astype(jnp.bfloat16)


def level_of(own_key, shape, cuts, low, high):
    factor_of, own = 1.0, jax.random.fold_in(own_key, 6)
    for position, blocks in cuts:
        steps = jnp.exp(jax.random.uniform(jax.random.fold_in(own, position), (blocks,), jnp.float32, low / len(cuts), high / len(cuts)))
        factor_of = factor_of * jnp.repeat(steps, shape[position] // blocks).reshape([-1 if axis == position else 1 for axis in range(len(shape))])
    return factor_of


def normal_values(stream_key, extent, scale, bound, cuts=(), kind=jnp.bfloat16):
    gain = level_of(stream_key, extent, cuts, -0.22, 0.18) if cuts else 1.0
    array = jax.random.normal(stream_key, extent, jnp.float32) * scale * gain
    return jnp.minimum(jnp.maximum(array, -bound), bound).astype(kind)


def setup_inputs(seed: int = 0) -> dict:
    splits = jax.random.split(jax.random.key(seed), 12)
    resid = normal_values(splits[0], (TOKENS, D), 1.0, 6.0, ((0, 16),))
    queries = draw_queries(jax.random.fold_in(splits[11], 71), 0)
    keys = draw_keys(jax.random.fold_in(splits[11], 71), 0)
    values = normal_values(splits[3], (TOKENS, HEADS * VD), 1.0, 6.0, ((0, 16), (1, 2)))
    lambdas = jnp.clip(0.3 + 0.5 * jax.random.uniform(splits[4], (HEADS,), jnp.float32) ** level_of(splits[4], (HEADS,), ((0, 2),), -0.2, 0.2), 0.3, 0.8)
    head_gain = jnp.clip(1.0 + 0.18 * jax.random.normal(splits[5], (VD,), jnp.float32), 0.1, 1.9)
    out_weight = normal_values(splits[6], (HEADS * VD, D), (HEADS * VD) ** -0.5, 0.1875, ((0, 2),))
    norm_gain = jnp.clip(1.0 + 0.18 * jax.random.normal(splits[7], (D,), jnp.float32), 0.1, 1.9)
    gate_weight = normal_values(splits[8], (D, FF), D ** -0.5, 0.125, ((0, 16), (1, 2)))
    up_weight = normal_values(splits[9], (D, FF), D ** -0.5, 0.125, ((0, 16), (1, 2)))
    down_weight = normal_values(splits[10], (FF, D), FF ** -0.5, 0.078125, ((0, 2), (1, 16)))
    return dict(resid=resid, queries=queries, keys=keys, values=values, lambdas=lambdas, head_gain=head_gain, out_weight=out_weight, norm_gain=norm_gain, gate_weight=gate_weight, up_weight=up_weight, down_weight=down_weight)


def reference(resid, queries, keys, values, lambdas, head_gain, out_weight, norm_gain, gate_weight, up_weight, down_weight):
    tok_total = resid.shape[0]
    head_count = lambdas.shape[0]
    query_all = queries.reshape(tok_total, head_count, 2, QK).astype(jnp.float32)
    key_all = keys.reshape(tok_total, head_count, 2, QK).astype(jnp.float32)
    value_all = values.reshape(tok_total, head_count, VD).astype(jnp.float32)
    score_scale = QK ** (-0.5)
    key_pos = jnp.arange(tok_total, dtype=jnp.int32)

    def one_block(block_index):
        block_start = (block_index * TOK_DEV).astype(jnp.int32)
        query_block = lax.dynamic_slice_in_dim(query_all, block_start, TOK_DEV, 0)
        scores = jnp.einsum('qhcd,khcd->chqk', query_block, key_all) * score_scale
        query_pos = block_start + jnp.arange(TOK_DEV, dtype=jnp.int32)
        causal_mask = key_pos[None, :] <= query_pos[:, None]
        scores = jnp.where(causal_mask, scores, -1e+30)
        row_max = lax.optimization_barrier(jnp.max(scores, axis=-1, keepdims=True))
        expo = jnp.where(causal_mask, jnp.exp(scores - row_max), 0.0)
        row_sum = lax.optimization_barrier(jnp.sum(expo, axis=-1))
        rounded = lax.optimization_barrier(expo.astype(jnp.bfloat16)).astype(jnp.float32)
        numer = jnp.einsum('chqk,khd->chqd', rounded, value_all)
        ratio = numer / row_sum[..., None]
        mixed_heads = ratio[0] - lambdas[:, None, None] * ratio[1]
        normed_heads = mixed_heads * lax.rsqrt(lax.optimization_barrier(jnp.mean(mixed_heads * mixed_heads, axis=-1, keepdims=True)) + 1e-05) * head_gain
        return jnp.transpose(normed_heads.astype(jnp.bfloat16), (1, 0, 2))
    head_out = lax.map(one_block, jnp.arange(tok_total // TOK_DEV, dtype=jnp.int32)).reshape(tok_total, head_count * VD)
    group_cols = head_count // N_TP * VD
    branch = jnp.zeros((tok_total, resid.shape[1]), jnp.float32)
    for group in range(N_TP):
        partial_sum = jnp.dot(head_out[:, group * group_cols:(group + 1) * group_cols], out_weight[group * group_cols:(group + 1) * group_cols], preferred_element_type=jnp.float32)
        branch = branch + partial_sum.astype(jnp.bfloat16).astype(jnp.float32)
    first = resid.astype(jnp.float32) + branch
    normed = (first * lax.rsqrt(lax.optimization_barrier(jnp.mean(first * first, axis=-1, keepdims=True)) + 1e-06) * norm_gain).astype(jnp.bfloat16)
    hidden_group = FF // N_TP
    mixer = jnp.zeros_like(first)
    for group in range(N_TP):
        cols = slice(group * hidden_group, (group + 1) * hidden_group)
        gate_act = jnp.dot(normed, gate_weight[:, cols], preferred_element_type=jnp.float32)
        up_act = jnp.dot(normed, up_weight[:, cols], preferred_element_type=jnp.float32)
        hidden = (jax.nn.silu(gate_act) * up_act).astype(jnp.bfloat16)
        partial_sum = jnp.dot(hidden, down_weight[cols, :], preferred_element_type=jnp.float32)
        mixer = mixer + partial_sum.astype(jnp.bfloat16).astype(jnp.float32)
    return (first + 0.5 * mixer).astype(jnp.bfloat16)
```

```python
import jax
import jax.numpy as jnp
from jax import lax
from jax.experimental import pallas as pl
from jax.experimental.pallas import tpu as pltpu
from jax.sharding import PartitionSpec as P

QK = 64
VD = 128
LANE = 128
SUB = 2
VMEM_LIMIT = 60 * 1024 * 1024


def rms_rows(first, norm_gain):
    return (
        first * lax.rsqrt(jnp.mean(first * first, axis=-1, keepdims=True) + 1e-06) * norm_gain
    ).astype(jnp.bfloat16)


def generic(
    resid,
    queries,
    keys,
    values,
    lambdas,
    head_gain,
    out_weight,
    norm_gain,
    gate_weight,
    up_weight,
    down_weight,
):
    tok_rows = queries.shape[0]
    local_heads = lambdas.shape[0]
    model_width = resid.shape[1]
    offset = lax.axis_index("sp") * tok_rows
    query_four = queries.reshape(tok_rows, local_heads, 2, QK)
    score_scale = QK ** (-0.5)
    query_pos = offset + lax.iota(jnp.int32, tok_rows)

    def update(fold_state, key_part, value_part, key_pos):
        run_max, run_sum, run_acc = fold_state
        scores = (
            jnp.einsum("qhcd,khcd->chqk", query_four, key_part, preferred_element_type=jnp.float32)
            * score_scale
        )
        causal_mask = key_pos[None, :] <= query_pos[:, None]
        scores = jnp.where(causal_mask, scores, -1e30)
        new_max = jnp.maximum(run_max, jnp.max(scores, axis=-1))
        expo = jnp.where(causal_mask, jnp.exp(scores - new_max[..., None]), 0.0)
        factor = jnp.exp(run_max - new_max)
        new_sum = run_sum * factor + jnp.sum(expo, axis=-1)
        new_acc = run_acc * factor[..., None] + jnp.einsum(
            "chqk,khd->chqd",
            expo.astype(jnp.bfloat16),
            value_part,
            preferred_element_type=jnp.float32,
        )
        return (new_max, new_sum, new_acc)

    initial = (
        jnp.full((2, local_heads, tok_rows), -1e30, jnp.float32),
        jnp.zeros((2, local_heads, tok_rows), jnp.float32),
        jnp.zeros((2, local_heads, tok_rows, VD), jnp.float32),
    )
    key_rows = lax.all_gather(keys, "sp", axis=0, tiled=True)
    value_rows = lax.all_gather(values, "sp", axis=0, tiled=True)
    key_count = key_rows.shape[0]
    key_span = key_count
    while key_span > 1024 and key_span % 2 == 0:
        key_span = key_span // 2

    def one_span(span_index, inner_state):
        span_start = span_index * key_span
        key_part = lax.dynamic_slice_in_dim(key_rows, span_start, key_span, 0).reshape(
            key_span, local_heads, 2, QK
        )
        value_part = lax.dynamic_slice_in_dim(value_rows, span_start, key_span, 0).reshape(
            key_span, local_heads, VD
        )
        key_pos = span_start + lax.iota(jnp.int32, key_span)
        return update(inner_state, key_part, value_part, key_pos)

    final_max, final_sum, final_acc = lax.fori_loop(0, key_count // key_span, one_span, initial)
    ratio = final_acc / final_sum[..., None]
    mixed_heads = ratio[0] - lambdas[:, None, None] * ratio[1]
    head_out = (
        mixed_heads
        * lax.rsqrt(jnp.mean(mixed_heads * mixed_heads, axis=-1, keepdims=True) + 1e-05)
        * head_gain
    ).astype(jnp.bfloat16)
    out_three = out_weight.reshape(local_heads, VD, model_width)
    own_count = tok_rows // lax.axis_size("tp")
    branch = lax.psum_scatter(
        jnp.einsum("hqd,hde->qe", head_out, out_three, preferred_element_type=jnp.float32).astype(
            jnp.bfloat16
        ),
        "tp",
        scatter_dimension=0,
        tiled=True,
    ).astype(jnp.float32)
    resid_own = lax.dynamic_slice_in_dim(resid, lax.axis_index("tp") * own_count, own_count, 0)
    first = resid_own.astype(jnp.float32) + branch
    normed_all = lax.all_gather(rms_rows(first, norm_gain), "tp", axis=0, tiled=True)
    gate_act = jnp.dot(
        normed_all,
        lax.all_gather(gate_weight, "sp", axis=0, tiled=True),
        preferred_element_type=jnp.float32,
    )
    up_act = jnp.dot(
        normed_all,
        lax.all_gather(up_weight, "sp", axis=0, tiled=True),
        preferred_element_type=jnp.float32,
    )
    hidden = (jax.nn.silu(gate_act) * up_act).astype(jnp.bfloat16)
    terms = jnp.dot(
        hidden,
        lax.all_gather(down_weight, "sp", axis=1, tiled=True),
        preferred_element_type=jnp.float32,
    )
    mixer = lax.psum_scatter(
        terms.astype(jnp.bfloat16), "tp", scatter_dimension=0, tiled=True
    ).astype(jnp.float32)
    finished = (first + 0.5 * mixer).astype(jnp.bfloat16)
    return lax.all_gather(finished, "tp", axis=0, tiled=True)


def where_am_i(R):
    s = lax.axis_index("sp")
    return s // R, lax.rem(s, R), lax.axis_index("tp")


def remote(src, dst, send, recv, sp, tp):
    return pltpu.make_async_remote_copy(
        src_ref=src,
        dst_ref=dst,
        send_sem=send,
        recv_sem=recv,
        device_id={"sp": sp, "tp": tp},
        device_id_type=pl.DeviceIdType.MESH,
    )


def greet(peers):
    barrier = pltpu.get_barrier_semaphore()
    for sp, tp in peers:
        pl.semaphore_signal(
            barrier,
            inc=1,
            device_id={"sp": sp, "tp": tp},
            device_id_type=pl.DeviceIdType.MESH,
        )
    pl.semaphore_wait(barrier, len(peers))


def mirror_x(r):
    return r + 1 - 2 * lax.rem(r, 2)


def mirror_y(r):
    return r + 2 - 4 * (lax.rem(r, 4) // 2)


def attention_block(R, T, i, r, q_at, k_at, v_at, lam, gain):
    span = R * T
    query = q_at(i) * jnp.bfloat16(QK**-0.5)
    ratios = []
    for c in range(2):
        part = query[:, c * QK : (c + 1) * QK]

        def fold(n, state, masked):
            run_max, run_sum, run_acc = state
            key = k_at(n)[:, c * QK : (c + 1) * QK]
            scores = lax.dot_general(
                part, key, (((1,), (1,)), ((), ())), preferred_element_type=jnp.float32
            )
            if masked:
                qpos = r * T + lax.broadcasted_iota(jnp.int32, scores.shape, 0)
                kpos = lax.broadcasted_iota(jnp.int32, scores.shape, 1)
                scores = jnp.where(kpos <= qpos, scores, -1e30)
            new_max = jnp.maximum(run_max, jnp.max(scores, axis=-1, keepdims=True))
            expo = jnp.exp(scores - new_max)
            factor = jnp.exp(run_max - new_max)
            new_sum = run_sum * factor + jnp.sum(expo, axis=-1, keepdims=True)
            new_acc = run_acc * factor + jnp.dot(
                expo.astype(jnp.bfloat16), v_at(n), preferred_element_type=jnp.float32
            )
            return new_max, new_sum, new_acc

        state = (
            jnp.full((T, 1), -1e30, jnp.float32),
            jnp.zeros((T, 1), jnp.float32),
            jnp.zeros((T, VD), jnp.float32),
        )
        state = fold(i, state, True)
        state = lax.fori_loop(0, i, lambda n, st: fold(n, st, False), state)
        ratios.append(state[2] / state[1])
    mixed = ratios[0] - lam * ratios[1]
    return (
        mixed * lax.rsqrt(jnp.mean(mixed * mixed, axis=-1, keepdims=True) + 1e-05) * gain
    ).astype(jnp.bfloat16)


def block_start(blocks, Z, zz, tt):
    return (blocks * zz + (1 - tt) * (Z // 2)) // Z


def when(cond, body):
    if cond is None:
        body()
    else:
        pl.when(cond)(body)


def whole_kernel(Z, R, blocks, pairs, singles, refs):
    (
        q_in, k_in, v_in, g_in, u_in, d_in, resid_in, w_in, lam, head_gain, norm_gain,
        out,
        q_sc, kv_sc, wide_sc, thin_sc, resid, w,
        ho, heads, part, got, first, norm_sc, all_sc,
        hidden, acc, half, cross, rs_out, rs_in, res,
        zs, zr, ps, pr, pl_sem, local_sem, ho_sem, swap_sem, ag_sem, core_sem,
        cross_sem, rs_sem, out_sem,
    ) = refs
    z, r, t = where_am_i(R)
    me = z * R + r
    rx, ry = mirror_x(r), mirror_y(r)
    rd = mirror_x(ry)
    T = k_in.shape[0]
    D = resid_in.shape[1]
    DN = d_in.shape[1]
    H = T // 2
    ahead = [lax.rem(z + j, Z) for j in range(Z)]
    behind = [lax.rem(z + Z - j, Z) for j in range(Z)]
    chunks = pairs + singles
    uneven = blocks % Z != 0
    Q, KV = chunks, chunks + 1

    def dev(zz, rr):
        return zz * R + rr

    def span_of(c):
        return 2 if c < pairs else 1

    def offset(c):
        return 2 * c if c < pairs else pairs + c

    def store(o):
        if o == Q:
            return q_sc
        if o == KV:
            return kv_sc
        return wide_sc.at[o] if o < pairs else thin_sc.at[o - pairs]

    def present(o, zz):
        if not uneven or o != chunks - 1:
            return None
        count = block_start(blocks, Z, zz + 1, t) - block_start(blocks, Z, zz, t)
        return count > blocks // Z

    here = [present(o, z) for o in range(chunks + 2)]

    def parts(o, zz, slot):
        if o >= chunks:
            cols = pl.ds(pl.multiple_of(zz * VD, LANE), VD)
            if o == Q:
                return [(q_in.at[:, cols], q_sc.at[slot])]
            return [
                (ref.at[:, cols], kv_sc.at[slot, :, pl.ds(i * VD, VD)])
                for i, ref in enumerate((k_in, v_in))
            ]
        n = span_of(o)
        dst = store(o)
        start = pl.multiple_of((block_start(blocks, Z, zz, t) + offset(o)) * LANE, LANE)
        pairs_ = [
            (ref.at[:, pl.ds(start, n * LANE)], dst.at[slot, :, pl.ds(i * n * LANE, n * LANE)])
            for i, ref in enumerate((g_in, u_in))
        ]
        for i in range(n):
            rows = pl.ds(pl.multiple_of(start + i * LANE, LANE), LANE)
            pairs_.append((d_in.at[rows, :], dst.at[slot, :, pl.ds((2 * n + i) * LANE, LANE)]))
        return pairs_

    def slot_of(o, zz):
        return zz if o == Q else dev(zz, r)

    started = []

    def launch(cond, make):
        when(cond, lambda: make().start())
        started.append((cond, make))

    def zsend(o, j):
        return zs.at[o if here[o] is None else chunks + 1 + j]

    def first_hop(o, j):
        def body():
            for src, dst in parts(o, ahead[j], slot_of(o, z)):
                remote(src, dst, zsend(o, j), zr.at[o, j - 1], dev(ahead[j], r), t).start()

        when(present(o, ahead[j]), body)

    def arrived(o, j):
        spot = store(o).at[slot_of(o, behind[j])]

        def body():
            remote(spot, spot, zsend(o, j), zr.at[o, j - 1], dev(behind[j], r), t).wait_recv()

        when(here[o], body)

    def first_hops_sent(o):
        if here[o] is None:
            whole = store(o).at[pl.ds(0, Z - 1)]
            remote(whole, whole, zsend(o, 1), zr.at[o, 0], dev(ahead[1], r), t).wait_send()
            return
        for j in range(1, Z):
            spot = store(o).at[0]
            when(
                present(o, ahead[j]),
                lambda j=j: remote(
                    spot, spot, zsend(o, j), zr.at[o, j - 1], dev(ahead[j], r), t
                ).wait_send(),
            )

    def keep(o):
        def body():
            for src, dst in parts(o, z, slot_of(o, z)):
                pltpu.make_async_copy(src, dst, local_sem.at[o]).start()

        when(here[o], body)

    def kept(o):
        spot = store(o).at[slot_of(o, z)]
        when(here[o], lambda: pltpu.make_async_copy(spot, spot, local_sem.at[o]).wait())

    def piece(o, j, owner, h):
        ref = store(o)
        n = ref.shape[1] // 2
        return ref.at[dev(behind[j], owner), pl.ds(h * n, n), :]

    def psem(o):
        return o if o < chunks else chunks

    def landing(o, j, kind):
        p = psem(o)
        return pr.at[p, j, 0 if kind == 0 else 1] if kind in (0, 3) else pl_sem.at[p]

    def hop2(o, j, kind):
        owner = (r, r, r, r, rx, ry)[kind]
        target = (rx, rx, ry, ry, ry, rx)[kind]
        spot = piece(o, j, owner, kind % 2)
        return remote(spot, spot, ps.at[psem(o)], landing(o, j, kind), dev(z, target), t)

    def wait2(o, j, kind):
        owner = rx if kind == 0 else ry
        spot = piece(o, j, owner, kind % 2)
        remote(spot, spot, ps.at[psem(o)], landing(o, j, kind), dev(z, owner), t).wait_recv()

    def spread(o, j):
        if j:
            arrived(o, j)
        else:
            kept(o)

        def body():
            for kind in (0, 3, 1, 2):
                hop2(o, j, kind).start()

        when(here[o], body)

    def relay(o, j):
        def body():
            wait2(o, j, 0)
            hop2(o, j, 4).start()
            wait2(o, j, 3)
            hop2(o, j, 5).start()

        when(here[o], body)

    def settle(o):
        whole = store(o).at[pl.ds(0, 2 * Z)]
        when(
            here[o],
            lambda: remote(
                whole, whole, ps.at[psem(o)], landing(o, 0, 1), dev(z, rx), t
            ).wait_recv(),
        )

    def spread_sent(o):
        whole = store(o).at[pl.ds(0, 3 * Z)]
        when(
            here[o],
            lambda: remote(
                whole, whole, ps.at[psem(o)], landing(o, 0, 1), dev(z, rx), t
            ).wait_send(),
        )

    for o in (KV, *range(chunks), Q):
        keep(o)
    resid_copy = pltpu.make_async_copy(resid_in, resid, local_sem.at[chunks + 2])
    resid_copy.start()
    w_copy = pltpu.make_async_copy(w_in, w, local_sem.at[chunks + 3])
    w_copy.start()

    greet(
        [(dev(ahead[j], r), t) for j in range(1, Z)]
        + [(dev(z, rx), t), (dev(z, ry), t), (me, 1 - t)]
    )
    for o in (KV, Q, 0, 1):
        for j in range(1, Z):
            first_hop(o, j)
        if o == KV:
            spread(KV, 0)
    spread(0, 0)
    relay(KV, 0)
    for j in range(1, Z):
        spread(KV, j)
        if j > 1:
            relay(KV, j - 1)
    relay(0, 0)
    relay(KV, Z - 1)
    for c in range(1, chunks):
        spread(c, 0)
    settle(KV)
    kept(Q)
    for j in range(1, Z):
        arrived(Q, j)

    head_lam = lam[z]

    def span(n, first_lane):
        return kv_sc[pl.ds(n * R, R), :, first_lane : first_lane + VD].reshape(R * T, VD)

    def ho_copy(i):
        return remote(ho.at[i], heads.at[z], ho_sem.at[0, i], ho_sem.at[1, z], dev(i, r), t)

    for i in range(Z):
        ho[i] = attention_block(
            R, T, i, r,
            lambda b: q_sc[b],
            lambda n: span(n, 0),
            lambda n: span(n, VD),
            head_lam,
            head_gain[...],
        )

        @pl.when(z == i)
        def _(i=i):
            heads[i] = ho[i]

        launch(z != i, lambda i=i: ho_copy(i))
        if i < Z - 1:
            if i:
                relay(i, 0)
            spread(0, i + 1)
    relay(3, 0)
    spread(1, 1)
    relay(0, 1)
    resid_copy.wait()
    w_copy.wait()
    for i in range(Z):

        @pl.when(z != i)
        def _(i=i):
            remote(
                ho.at[i], heads.at[i], ho_sem.at[0, i], ho_sem.at[1, i], dev(i, r), t
            ).wait_recv()

    NT = 512 if D % 512 == 0 else D
    for h in range(2):
        hh = (1 - t) if h == 0 else t
        rows = pl.ds(pl.multiple_of(hh * H, 16), H)
        left = jnp.concatenate([heads[n, rows, :] for n in range(Z)], axis=1)
        for n in range(0, D, NT):
            part[h, :, n : n + NT] = jnp.dot(
                left, w[:, n : n + NT], preferred_element_type=jnp.float32
            ).astype(jnp.bfloat16)
        if h == 0:
            swap = remote(part.at[0], got, swap_sem.at[0], swap_sem.at[1], me, 1 - t)
            swap.start()
    swap.wait()
    own_rows = pl.ds(pl.multiple_of(t * H, 16), H)
    first_val = resid[own_rows, :].astype(jnp.float32) + (
        part[1].astype(jnp.float32) + got[...].astype(jnp.float32)
    )
    first[...] = first_val
    norm_sc[...] = rms_rows(first_val, norm_gain[...])

    def rows_of(zz, tt):
        return all_sc.at[zz, tt]

    def ag_hop(down, d):
        zz = z + (d - 1) if down else z - (d - 1)
        to = z - 1 if down else z + 1
        return remote(
            norm_sc if d == 1 else rows_of(zz, t),
            rows_of(zz, t),
            ag_sem.at[2 * down, d],
            ag_sem.at[2 * down + 1, d],
            dev(to, r),
            t,
        )

    def sends(down, d):
        return (z > 0) & (z + (d - 1) < Z) if down else (z + 1 < Z) & (z - (d - 1) >= 0)

    def gets(down, d):
        return z + d < Z if down else z - d >= 0

    def origin(down, d):
        return z + d if down else z - d

    def to_core(down, d, tt):
        rows = rows_of(origin(down, d), tt)
        n = 2 * d + down
        return remote(rows, rows, core_sem.at[0, n], core_sem.at[1, n], me, 1 - t)

    def ag_start(d):
        for down in (0, 1):

            @pl.when(sends(down, d))
            def _(down=down):
                ag_hop(down, d).start()

    def ag_step(d):
        for down in (0, 1):

            @pl.when(gets(down, d))
            def _(down=down):
                rows = rows_of(origin(down, d), t)
                remote(
                    rows, rows, ag_sem.at[2 * down, d], ag_sem.at[2 * down + 1, d], me, 1 - t
                ).wait_recv()
                if d < Z - 1:

                    @pl.when(sends(down, d + 1))
                    def _():
                        ag_hop(down, d + 1).start()

                to_core(down, d, t).start()

    def ag_done(d):
        for down in (0, 1):

            @pl.when(gets(down, d))
            def _(down=down):
                to_core(down, d, 1 - t).wait_recv()

    def apply(cs, zz, fresh):
        block = all_sc[zz].reshape(T, D)
        lane = 0
        for c in cs:
            n = span_of(c) * LANE
            both = jnp.dot(
                block,
                store(c)[:, :, : 2 * n].reshape(D, 2 * n),
                preferred_element_type=jnp.float32,
            )
            value = jax.nn.silu(both[:, :n]) * both[:, n:]
            hidden[:, lane : lane + n] = value.astype(jnp.bfloat16)
            lane += n
        left = hidden[:, :lane]
        spots = [(c, 2 * span_of(c) + i) for c in cs for i in range(span_of(c))]
        group = 4 if (Z * R) % 8 == 0 else 1

        @pl.loop(0, (Z * R) // (2 * group))
        def _(g):
            for q in range(group):
                p = g * group + q
                right = jnp.concatenate(
                    [
                        jnp.concatenate(
                            [store(c)[2 * p + i, :, k * LANE : (k + 1) * LANE] for c, k in spots],
                            axis=0,
                        )
                        for i in range(2)
                    ],
                    axis=1,
                )
                value = jnp.dot(left, right, preferred_element_type=jnp.float32)
                cols = pl.ds(pl.multiple_of(p * (2 * DN), 2 * DN), 2 * DN)
                if fresh:
                    acc[zz, :, cols] = value
                else:
                    acc[zz, :, cols] = acc[zz, :, cols] + value

    early = tuple(range(pairs))
    late = tuple(range(pairs, chunks))

    def apply_last(cs, zz, fresh):
        cond = here[chunks - 1]
        if cond is None:
            apply(cs, zz, fresh)
            return
        pl.when(cond)(lambda: apply(cs, zz, fresh))
        if cs[:-1]:
            pl.when(jnp.logical_not(cond))(lambda: apply(cs[:-1], zz, fresh))

    def apply_near(cs, d, fresh):
        for down in (0, 1):

            @pl.when(gets(down, d))
            def _(down=down):
                apply(cs, origin(down, d), fresh)

    ag_start(1)
    across = remote(norm_sc, rows_of(z, t), core_sem.at[0, 0], core_sem.at[1, 0], me, 1 - t)
    across.start()
    own = pltpu.make_async_copy(norm_sc, rows_of(z, t), local_sem.at[0])
    own.start()
    for c in range(2, chunks):
        for j in range(1, Z):
            first_hop(c, j)
    spread(1, 2)
    relay(0, 2)
    spread(1, 3)
    relay(0, 3)
    relay(1, 1)
    ag_step(1)
    own.wait()
    across.wait_send()
    remote(
        norm_sc, rows_of(z, 1 - t), core_sem.at[0, 0], core_sem.at[1, 0], me, 1 - t
    ).wait_recv()
    relay(1, 2)
    relay(1, 3)
    for c in late:
        for j in range(1, Z):
            spread(c, j)
    for c in early:
        settle(c)
    apply(early, z, True)
    ag_done(1)
    apply_near(early, 1, True)
    for j in range(1, Z):
        relay(2, j)
    ag_step(2)
    for j in range(1, Z):
        relay(3, j)
    ag_done(2)
    apply_near(early, 2, True)
    for c in late:
        settle(c)

    def pick(table):
        spot = jnp.int32(0)
        for zz in range(Z):
            spot = jnp.where(z == zz, table[zz], spot)
        return spot

    goals = [[Z - 2, Z - 1] + list(range(Z - 3, 0, -1)), [1, 0] + list(range(2, Z - 1))]
    ranks = []
    for zz in range(Z):
        seq = []
        for k in range(Z - 1):
            for down in (0, 1):
                zd = goals[down][k]
                if (zz > zd if down else zz < zd) and zd not in seq:
                    seq.append(zd)
        ranks.append(seq + [zz])

    def cross_copy(zz):
        return remote(
            half.at[zz], cross.at[zz], cross_sem.at[0, zz], cross_sem.at[1, zz], me, 1 - t
        )

    other_rows = pl.ds(pl.multiple_of((1 - t) * H, 16), H)
    piece = H // SUB

    def rs_copy(down, k, s):
        rows = pl.ds(s * piece, piece)
        to = z - 1 if down else z + 1
        return remote(
            rs_out.at[down, k, rows],
            rs_in.at[down, k, rows],
            rs_sem.at[2 * down, k, s],
            rs_sem.at[2 * down + 1, k, s],
            dev(to, r),
            t,
        )

    def rs_wait(down, k, s):
        rows = pl.ds(s * piece, piece)
        fro = z + 1 if down else z - 1
        remote(
            rs_out.at[down, k, rows],
            rs_in.at[down, k, rows],
            rs_sem.at[2 * down, k, s],
            rs_sem.at[2 * down + 1, k, s],
            dev(fro, r),
            t,
        ).wait_recv()

    def mine(zd, s):
        rows = pl.ds(s * piece, piece)
        long = pl.ds(pl.multiple_of(t * H + s * piece, 16), piece)
        return acc[zd, long, :] + cross[zd, rows, :].astype(jnp.float32)

    def hand_over(zz):
        half[zz] = acc[zz, other_rows, :].astype(jnp.bfloat16)
        cross_copy(zz).start()

    def rs_step(down, k, inner):
        zd = goals[down][k]
        for s in range(SUB):
            rows = pl.ds(s * piece, piece)
            if s == 0:
                cross_copy(zd).wait_recv()
            total = mine(zd, s)
            if inner:
                rs_wait(down, k, s)
                total = total + rs_in[down, k, rows, :].astype(jnp.float32)
            rs_out[down, k, rows, :] = total.astype(jnp.bfloat16)
            rs_copy(down, k, s).start()

    for n in range(Z):
        zz = pick([ranks[i][n] for i in range(Z)])
        if n == 1:
            for d in range(3, Z):
                ag_step(d)
                ag_done(d)
            edge = (z == 0) | (z == Z - 1)
            pl.when(edge)(lambda: apply_last(early + late, zz, True))
            pl.when(jnp.logical_not(edge))(lambda: apply_last(late, zz, False))
        else:
            apply_last(late, zz, False)
        hand_over(zz)
        if n < Z - 1:
            pl.when(z == 0)(lambda: rs_step(0, n, False))
            pl.when(z == Z - 1)(lambda: rs_step(1, n, False))
    for k in range(Z - 1):
        for down in (0, 1):
            zd = goals[down][k]
            inner = (z > zd) & (z < Z - 1) if down else (z < zd) & (z > 0)
            pl.when(inner)(lambda: rs_step(down, k, True))
    cross_copy(z).wait_recv()
    ends = []
    for s in range(SUB):
        rows = pl.ds(s * piece, piece)
        first[rows, :] = first[rows, :] + 0.5 * mine(z, s)
        for down in (0, 1):

            @pl.when(z < Z - 1 if down else z > 0)
            def _(down=down, s=s, rows=rows):
                k = pick([goals[down].index(i) if i in goals[down] else 0 for i in range(Z)])
                rs_wait(down, k, s)
                first[rows, :] = first[rows, :] + 0.5 * rs_in[down, k, rows, :].astype(jnp.float32)

        res[rows, :] = first[rows, :].astype(jnp.bfloat16)
        place = out.at[pl.ds(pl.multiple_of(t * H + s * piece, 16), piece), :]
        c = remote(res.at[rows], place, out_sem.at[0, s], out_sem.at[1, s], me, 1 - t)
        c.start()
        ends.append(c)
        c = pltpu.make_async_copy(res.at[rows], place, local_sem.at[1 + s])
        c.start()
        ends.append(c)
    for c in ends:
        c.wait()
    for zz in range(Z):
        cross_copy(zz).wait_send()
    for d in range(1, Z):
        for down in (0, 1):

            @pl.when(gets(down, d))
            def _(down=down, d=d):
                to_core(down, d, t).wait_send()

            @pl.when(sends(down, d))
            def _(down=down, d=d):
                ag_hop(down, d).wait_send()

    for k in range(Z - 1):
        for down in (0, 1):
            zd = goals[down][k]

            @pl.when(z > zd if down else z < zd)
            def _(down=down, k=k):
                for s in range(SUB):
                    rs_copy(down, k, s).wait_send()

    for o in (KV, Q, *range(chunks)):
        first_hops_sent(o)
    for o in (KV, *range(chunks)):
        spread_sent(o)
    for cond, make in started:
        when(cond, lambda make=make: make().wait_send())


def columns_form(
    resid,
    queries,
    keys,
    values,
    lambdas,
    head_gain,
    out_weight,
    norm_gain,
    gate_weight,
    up_weight,
    down_weight,
):
    Z = lambdas.shape[0]
    S = lax.axis_size("sp")
    R = S // Z
    T, D = resid.shape
    H = T // 2
    W = gate_weight.shape[0]
    DN = down_weight.shape[1]
    blocks = gate_weight.shape[1] // LANE
    pairs = blocks // Z // 2
    singles = blocks // Z % 2 + (1 if blocks % Z else 0)
    chunks = pairs + singles
    bf, f32 = jnp.bfloat16, jnp.float32
    vm = pl.BlockSpec(memory_space=pltpu.VMEM)
    hbm = pl.BlockSpec(memory_space=pl.ANY)
    dma = pltpu.SemaphoreType.DMA

    def kernel(*refs):
        whole_kernel(Z, R, blocks, pairs, singles, refs)

    return pl.pallas_call(
        kernel,
        out_shape=jax.ShapeDtypeStruct((T, D), bf),
        in_specs=[hbm] * 8 + [pl.BlockSpec(memory_space=pltpu.SMEM), vm, vm],
        out_specs=vm,
        scratch_shapes=[
            pltpu.VMEM((Z, T, VD), bf),
            pltpu.VMEM((S, T, 2 * VD), bf),
            pltpu.VMEM((pairs, S, W, 6 * LANE), bf),
            pltpu.VMEM((singles, S, W, 3 * LANE), bf),
            pltpu.VMEM((T, D), bf),
            pltpu.VMEM(out_weight.shape, bf),
            pltpu.VMEM((Z, T, VD), bf),
            pltpu.VMEM((Z, T, VD), bf),
            pltpu.VMEM((2, H, D), bf),
            pltpu.VMEM((H, D), bf),
            pltpu.VMEM((H, D), f32),
            pltpu.VMEM((H, D), bf),
            pltpu.VMEM((Z, 2, H, D), bf),
            pltpu.VMEM((T, (2 * pairs + singles) * LANE), bf),
            pltpu.VMEM((Z, T, D), f32),
            pltpu.VMEM((Z, H, D), bf),
            pltpu.VMEM((Z, H, D), bf),
            pltpu.VMEM((2, Z - 1, H, D), bf),
            pltpu.VMEM((2, Z - 1, H, D), bf),
            pltpu.VMEM((H, D), bf),
            dma((chunks + 1 + Z,)),
            dma((chunks + 2, Z - 1)),
            dma((chunks + 1,)),
            dma((chunks + 1, Z, 2)),
            dma((chunks + 1,)),
            dma((chunks + 4,)),
            dma((2, Z)),
            dma((2,)),
            dma((4, Z)),
            dma((2, 2 * Z)),
            dma((2, Z)),
            dma((4, Z - 1, SUB)),
            dma((2, SUB)),
        ],
        compiler_params=pltpu.CompilerParams(
            collective_id=0, has_side_effects=True, vmem_limit_bytes=VMEM_LIMIT
        ),
    )(
        queries,
        keys,
        values,
        gate_weight,
        up_weight,
        down_weight,
        resid,
        out_weight,
        lambdas,
        head_gain.reshape(1, -1),
        norm_gain.reshape(1, -1),
    )


def solution(mesh):
    sp, tp = mesh.shape["sp"], mesh.shape["tp"]

    def local(*args):
        heads = args[4].shape[0]
        tok_rows = args[1].shape[0]
        columns = (
            tp == 2
            and heads == 4
            and sp == 4 * heads
            and args[10].shape[1] == LANE
            and args[8].shape[0] == LANE
            and args[8].shape[1] % LANE == 0
            and args[8].shape[1] // LANE // heads == 5
            and args[8].shape[1] // LANE % heads != 0
            and tok_rows % (32 * SUB) == 0
        )
        return (columns_form if columns else generic)(*args)

    return jax.shard_map(
        local,
        mesh=mesh,
        in_specs=(
            P("sp", None),
            P("sp", "tp"),
            P("sp", "tp"),
            P("sp", "tp"),
            P("tp"),
            P(),
            P("tp", None),
            P(),
            P("sp", "tp"),
            P("sp", "tp"),
            P("tp", "sp"),
        ),
        out_specs=P("sp", None),
        check_vma=False,
    )
```

```python
import jax
import jax.numpy as jnp
from jax import lax
from jax.experimental import pallas as pl
from jax.experimental.pallas import tpu as pltpu
from jax.sharding import PartitionSpec as P

QK = 64
VD = 128
LANE = 128
SUB = 3
VMEM_LIMIT = 60 * 1024 * 1024


def rms_rows(first, norm_gain):
    return (
        first * lax.rsqrt(jnp.mean(first * first, axis=-1, keepdims=True) + 1e-06) * norm_gain
    ).astype(jnp.bfloat16)


def generic(
    resid,
    queries,
    keys,
    values,
    lambdas,
    head_gain,
    out_weight,
    norm_gain,
    gate_weight,
    up_weight,
    down_weight,
):
    tok_rows = queries.shape[0]
    local_heads = lambdas.shape[0]
    model_width = resid.shape[1]
    offset = lax.axis_index("sp") * tok_rows
    query_four = queries.reshape(tok_rows, local_heads, 2, QK)
    score_scale = QK ** (-0.5)
    query_pos = offset + lax.iota(jnp.int32, tok_rows)

    def update(fold_state, key_part, value_part, key_pos):
        run_max, run_sum, run_acc = fold_state
        scores = (
            jnp.einsum("qhcd,khcd->chqk", query_four, key_part, preferred_element_type=jnp.float32)
            * score_scale
        )
        causal_mask = key_pos[None, :] <= query_pos[:, None]
        scores = jnp.where(causal_mask, scores, -1e30)
        new_max = jnp.maximum(run_max, jnp.max(scores, axis=-1))
        expo = jnp.where(causal_mask, jnp.exp(scores - new_max[..., None]), 0.0)
        factor = jnp.exp(run_max - new_max)
        new_sum = run_sum * factor + jnp.sum(expo, axis=-1)
        new_acc = run_acc * factor[..., None] + jnp.einsum(
            "chqk,khd->chqd",
            expo.astype(jnp.bfloat16),
            value_part,
            preferred_element_type=jnp.float32,
        )
        return (new_max, new_sum, new_acc)

    initial = (
        jnp.full((2, local_heads, tok_rows), -1e30, jnp.float32),
        jnp.zeros((2, local_heads, tok_rows), jnp.float32),
        jnp.zeros((2, local_heads, tok_rows, VD), jnp.float32),
    )
    key_rows = lax.all_gather(keys, "sp", axis=0, tiled=True)
    value_rows = lax.all_gather(values, "sp", axis=0, tiled=True)
    key_count = key_rows.shape[0]
    key_span = key_count
    while key_span > 1024 and key_span % 2 == 0:
        key_span = key_span // 2

    def one_span(span_index, inner_state):
        span_start = span_index * key_span
        key_part = lax.dynamic_slice_in_dim(key_rows, span_start, key_span, 0).reshape(
            key_span, local_heads, 2, QK
        )
        value_part = lax.dynamic_slice_in_dim(value_rows, span_start, key_span, 0).reshape(
            key_span, local_heads, VD
        )
        key_pos = span_start + lax.iota(jnp.int32, key_span)
        return update(inner_state, key_part, value_part, key_pos)

    final_max, final_sum, final_acc = lax.fori_loop(0, key_count // key_span, one_span, initial)
    ratio = final_acc / final_sum[..., None]
    mixed_heads = ratio[0] - lambdas[:, None, None] * ratio[1]
    head_out = (
        mixed_heads
        * lax.rsqrt(jnp.mean(mixed_heads * mixed_heads, axis=-1, keepdims=True) + 1e-05)
        * head_gain
    ).astype(jnp.bfloat16)
    out_three = out_weight.reshape(local_heads, VD, model_width)
    own_count = tok_rows // lax.axis_size("tp")
    branch = lax.psum_scatter(
        jnp.einsum("hqd,hde->qe", head_out, out_three, preferred_element_type=jnp.float32).astype(
            jnp.bfloat16
        ),
        "tp",
        scatter_dimension=0,
        tiled=True,
    ).astype(jnp.float32)
    resid_own = lax.dynamic_slice_in_dim(resid, lax.axis_index("tp") * own_count, own_count, 0)
    first = resid_own.astype(jnp.float32) + branch
    normed_all = lax.all_gather(rms_rows(first, norm_gain), "tp", axis=0, tiled=True)
    gate_act = jnp.dot(
        normed_all,
        lax.all_gather(gate_weight, "sp", axis=0, tiled=True),
        preferred_element_type=jnp.float32,
    )
    up_act = jnp.dot(
        normed_all,
        lax.all_gather(up_weight, "sp", axis=0, tiled=True),
        preferred_element_type=jnp.float32,
    )
    hidden = (jax.nn.silu(gate_act) * up_act).astype(jnp.bfloat16)
    terms = jnp.dot(
        hidden,
        lax.all_gather(down_weight, "sp", axis=1, tiled=True),
        preferred_element_type=jnp.float32,
    )
    mixer = lax.psum_scatter(
        terms.astype(jnp.bfloat16), "tp", scatter_dimension=0, tiled=True
    ).astype(jnp.float32)
    finished = (first + 0.5 * mixer).astype(jnp.bfloat16)
    return lax.all_gather(finished, "tp", axis=0, tiled=True)


def where_am_i(R):
    s = lax.axis_index("sp")
    return s // R, lax.rem(s, R), lax.axis_index("tp")


def remote(src, dst, send, recv, sp, tp):
    return pltpu.make_async_remote_copy(
        src_ref=src,
        dst_ref=dst,
        send_sem=send,
        recv_sem=recv,
        device_id={"sp": sp, "tp": tp},
        device_id_type=pl.DeviceIdType.MESH,
    )


def greet(peers):
    barrier = pltpu.get_barrier_semaphore()
    for sp, tp in peers:
        pl.semaphore_signal(
            barrier,
            inc=1,
            device_id={"sp": sp, "tp": tp},
            device_id_type=pl.DeviceIdType.MESH,
        )
    pl.semaphore_wait(barrier, len(peers))


def mirror_x(r):
    return r + 1 - 2 * lax.rem(r, 2)


def mirror_y(r):
    return r + 2 - 4 * (lax.rem(r, 4) // 2)


def attention_block(R, T, i, r, q_at, k_at, v_at, lam, gain):
    span = R * T
    query = q_at(i) * jnp.bfloat16(QK**-0.5)
    ratios = []
    for c in range(2):
        part = query[:, c * QK : (c + 1) * QK]

        def fold(n, state, masked):
            run_max, run_sum, run_acc = state
            key = k_at(n)[:, c * QK : (c + 1) * QK]
            scores = lax.dot_general(
                part, key, (((1,), (1,)), ((), ())), preferred_element_type=jnp.float32
            )
            if masked:
                qpos = r * T + lax.broadcasted_iota(jnp.int32, scores.shape, 0)
                kpos = lax.broadcasted_iota(jnp.int32, scores.shape, 1)
                scores = jnp.where(kpos <= qpos, scores, -1e30)
            new_max = jnp.maximum(run_max, jnp.max(scores, axis=-1, keepdims=True))
            expo = jnp.exp(scores - new_max)
            factor = jnp.exp(run_max - new_max)
            new_sum = run_sum * factor + jnp.sum(expo, axis=-1, keepdims=True)
            new_acc = run_acc * factor + jnp.dot(
                expo.astype(jnp.bfloat16), v_at(n), preferred_element_type=jnp.float32
            )
            return new_max, new_sum, new_acc

        state = (
            jnp.full((T, 1), -1e30, jnp.float32),
            jnp.zeros((T, 1), jnp.float32),
            jnp.zeros((T, VD), jnp.float32),
        )
        state = fold(i, state, True)
        state = lax.fori_loop(0, i, lambda n, st: fold(n, st, False), state)
        ratios.append(state[2] / state[1])
    mixed = ratios[0] - lam * ratios[1]
    return (
        mixed * lax.rsqrt(jnp.mean(mixed * mixed, axis=-1, keepdims=True) + 1e-05) * gain
    ).astype(jnp.bfloat16)


def block_start(blocks, Z, zz, tt):
    return (blocks * zz + (1 - tt) * (Z // 2)) // Z


def when(cond, body):
    if cond is None:
        body()
    else:
        pl.when(cond)(body)


def whole_kernel(Z, R, blocks, pairs, singles, refs):
    (
        q_in, k_in, v_in, g_in, u_in, d_in, resid_in, w_in, lam, head_gain, norm_gain,
        out,
        q_sc, kv_sc, wide_sc, thin_sc, resid, w,
        ho, heads, part, got, first, norm_sc, all_sc,
        hidden, acc, half, cross, rs_out, rs_in, res,
        zs, zr, ps, pr, pl_sem, local_sem, ho_sem, swap_sem, ag_sem, ag_land, core_sem,
        cross_sem, rs_sem, rs_land, out_sem,
    ) = refs
    z, r, t = where_am_i(R)
    me = z * R + r
    rx, ry = mirror_x(r), mirror_y(r)
    rd = mirror_x(ry)
    T = k_in.shape[0]
    D = resid_in.shape[1]
    DN = d_in.shape[1]
    H = T // 2
    ahead = [lax.rem(z + j, Z) for j in range(Z)]
    behind = [lax.rem(z + Z - j, Z) for j in range(Z)]
    chunks = pairs + singles
    uneven = blocks % Z != 0
    Q, KV = chunks, chunks + 1

    def dev(zz, rr):
        return zz * R + rr

    def span_of(c):
        return 2 if c < pairs else 1

    def offset(c):
        return 2 * c if c < pairs else pairs + c

    def store(o):
        if o == Q:
            return q_sc
        if o == KV:
            return kv_sc
        return wide_sc.at[o] if o < pairs else thin_sc.at[o - pairs]

    def present(o, zz):
        if not uneven or o != chunks - 1:
            return None
        count = block_start(blocks, Z, zz + 1, t) - block_start(blocks, Z, zz, t)
        return count > blocks // Z

    here = [present(o, z) for o in range(chunks + 2)]

    def parts(o, zz, slot):
        if o >= chunks:
            cols = pl.ds(pl.multiple_of(zz * VD, LANE), VD)
            if o == Q:
                return [(q_in.at[:, cols], q_sc.at[slot])]
            return [
                (ref.at[:, cols], kv_sc.at[slot, :, pl.ds(i * VD, VD)])
                for i, ref in enumerate((k_in, v_in))
            ]
        n = span_of(o)
        dst = store(o)
        start = pl.multiple_of((block_start(blocks, Z, zz, t) + offset(o)) * LANE, LANE)
        pairs_ = [
            (ref.at[:, pl.ds(start, n * LANE)], dst.at[slot, :, pl.ds(i * n * LANE, n * LANE)])
            for i, ref in enumerate((g_in, u_in))
        ]
        for i in range(n):
            rows = pl.ds(pl.multiple_of(start + i * LANE, LANE), LANE)
            pairs_.append((d_in.at[rows, :], dst.at[slot, :, pl.ds((2 * n + i) * LANE, LANE)]))
        return pairs_

    def slot_of(o, zz):
        return zz if o == Q else dev(zz, r)

    started = []

    def launch(cond, make):
        when(cond, lambda: make().start())
        started.append((cond, make))

    def zsend(o, j):
        return zs.at[o if here[o] is None else chunks + 1 + j]

    def first_hop(o, j):
        def body():
            for src, dst in parts(o, ahead[j], slot_of(o, z)):
                remote(src, dst, zsend(o, j), zr.at[o, j - 1], dev(ahead[j], r), t).start()

        when(present(o, ahead[j]), body)

    def arrived(o, j):
        spot = store(o).at[slot_of(o, behind[j])]

        def body():
            remote(spot, spot, zsend(o, j), zr.at[o, j - 1], dev(behind[j], r), t).wait_recv()

        when(here[o], body)

    def first_hops_sent(o):
        if here[o] is None:
            whole = store(o).at[pl.ds(0, Z - 1)]
            remote(whole, whole, zsend(o, 1), zr.at[o, 0], dev(ahead[1], r), t).wait_send()
            return
        for j in range(1, Z):
            spot = store(o).at[0]
            when(
                present(o, ahead[j]),
                lambda j=j: remote(
                    spot, spot, zsend(o, j), zr.at[o, j - 1], dev(ahead[j], r), t
                ).wait_send(),
            )

    def keep(o):
        def body():
            for src, dst in parts(o, z, slot_of(o, z)):
                pltpu.make_async_copy(src, dst, local_sem.at[o]).start()

        when(here[o], body)

    def kept(o):
        spot = store(o).at[slot_of(o, z)]
        when(here[o], lambda: pltpu.make_async_copy(spot, spot, local_sem.at[o]).wait())

    def piece(o, j, owner, h):
        ref = store(o)
        n = ref.shape[1] // 2
        return ref.at[dev(behind[j], owner), pl.ds(h * n, n), :]

    def psem(o):
        return o if o < chunks else chunks

    def landing(o, j, kind):
        p = psem(o)
        return pr.at[p, j, 0 if kind == 0 else 1] if kind in (0, 3) else pl_sem.at[p]

    def hop2(o, j, kind):
        owner = (r, r, r, r, rx, ry)[kind]
        target = (rx, rx, ry, ry, ry, rx)[kind]
        spot = piece(o, j, owner, kind % 2)
        return remote(spot, spot, ps.at[psem(o)], landing(o, j, kind), dev(z, target), t)

    def wait2(o, j, kind):
        owner = rx if kind == 0 else ry
        spot = piece(o, j, owner, kind % 2)
        remote(spot, spot, ps.at[psem(o)], landing(o, j, kind), dev(z, owner), t).wait_recv()

    def spread(o, j):
        if j:
            arrived(o, j)
        else:
            kept(o)

        def body():
            for kind in (0, 3, 1, 2):
                hop2(o, j, kind).start()

        when(here[o], body)

    def relay(o, j):
        def body():
            wait2(o, j, 0)
            hop2(o, j, 4).start()
            wait2(o, j, 3)
            hop2(o, j, 5).start()

        when(here[o], body)

    def settle(o):
        whole = store(o).at[pl.ds(0, 2 * Z)]
        when(
            here[o],
            lambda: remote(
                whole, whole, ps.at[psem(o)], landing(o, 0, 1), dev(z, rx), t
            ).wait_recv(),
        )

    def spread_sent(o):
        whole = store(o).at[pl.ds(0, 3 * Z)]
        when(
            here[o],
            lambda: remote(
                whole, whole, ps.at[psem(o)], landing(o, 0, 1), dev(z, rx), t
            ).wait_send(),
        )

    for o in (KV, *range(chunks), Q):
        keep(o)
    resid_copy = pltpu.make_async_copy(resid_in, resid, local_sem.at[chunks + 2])
    resid_copy.start()
    w_copy = pltpu.make_async_copy(w_in, w, local_sem.at[chunks + 3])
    w_copy.start()

    greet(
        [(dev(ahead[j], r), t) for j in range(1, Z)]
        + [(dev(z, rx), t), (dev(z, ry), t), (me, 1 - t)]
    )
    for o in (KV, Q, 0, 1):
        for j in range(1, Z):
            first_hop(o, j)
        if o == KV:
            spread(KV, 0)
    spread(0, 0)
    relay(KV, 0)
    for j in range(1, Z):
        spread(KV, j)
        if j > 1:
            relay(KV, j - 1)
        if j == Z - 2:
            spread(1, 0)
    relay(0, 0)
    relay(KV, Z - 1)
    for c in range(2, chunks):
        spread(c, 0)
    settle(KV)
    kept(Q)
    for j in range(1, Z):
        arrived(Q, j)

    head_lam = lam[z]

    def span(n, first_lane):
        return kv_sc[pl.ds(n * R, R), :, first_lane : first_lane + VD].reshape(R * T, VD)

    def ho_copy(i):
        return remote(ho.at[i], heads.at[z], ho_sem.at[0, i], ho_sem.at[1, z], dev(i, r), t)

    for i in range(Z):
        ho[i] = attention_block(
            R, T, i, r,
            lambda b: q_sc[b],
            lambda n: span(n, 0),
            lambda n: span(n, VD),
            head_lam,
            head_gain[...],
        )

        @pl.when(z == i)
        def _(i=i):
            heads[i] = ho[i]

        launch(z != i, lambda i=i: ho_copy(i))
        if i == 0:
            relay(1, 0)
            spread(0, 1)
        if i == 1:
            relay(2, 0)
            relay(3, 0)
        if i == 2:
            spread(0, 2)
            relay(0, 1)
    spread(0, 3)
    relay(0, 2)
    spread(1, 1)
    spread(1, 2)
    relay(0, 3)
    spread(1, 3)
    relay(1, 1)
    resid_copy.wait()
    w_copy.wait()
    for i in range(Z):

        @pl.when(z != i)
        def _(i=i):
            remote(
                ho.at[i], heads.at[i], ho_sem.at[0, i], ho_sem.at[1, i], dev(i, r), t
            ).wait_recv()

    first_hop(2, 1)
    first_hop(2, 2)
    NT = 512 if D % 512 == 0 else D
    for h in range(2):
        hh = (1 - t) if h == 0 else t
        rows = pl.ds(pl.multiple_of(hh * H, 16), H)
        left = jnp.concatenate([heads[n, rows, :] for n in range(Z)], axis=1)
        for n in range(0, D, NT):
            part[h, :, n : n + NT] = jnp.dot(
                left, w[:, n : n + NT], preferred_element_type=jnp.float32
            ).astype(jnp.bfloat16)
        if h == 0:
            swap = remote(part.at[0], got, swap_sem.at[0], swap_sem.at[1], me, 1 - t)
            swap.start()
    swap.wait()
    own_rows = pl.ds(pl.multiple_of(t * H, 16), H)
    first_val = resid[own_rows, :].astype(jnp.float32) + (
        part[1].astype(jnp.float32) + got[...].astype(jnp.float32)
    )
    first[...] = first_val
    norm_sc[...] = rms_rows(first_val, norm_gain[...])

    def rows_of(zz, tt):
        return all_sc.at[zz, tt]

    part_rows = H // SUB

    def ag_hop(down, d, s=None):
        zz = z + (d - 1) if down else z - (d - 1)
        to = z - 1 if down else z + 1
        src = norm_sc if d == 1 else rows_of(zz, t)
        dst = rows_of(zz, t)
        if s is not None:
            src, dst = (ref.at[pl.ds(s * part_rows, part_rows)] for ref in (src, dst))
        return remote(
            src, dst, ag_sem.at[down, d], ag_land.at[down, d, 0 if s is None else s], dev(to, r), t
        )

    def sends(down, d):
        return (z > 0) & (z + (d - 1) < Z) if down else (z + 1 < Z) & (z - (d - 1) >= 0)

    def gets(down, d):
        return z + d < Z if down else z - d >= 0

    def origin(down, d):
        return z + d if down else z - d

    def to_core(down, d, tt):
        rows = rows_of(origin(down, d), tt)
        n = 2 * d + down
        return remote(rows, rows, core_sem.at[0, n], core_sem.at[1, n], me, 1 - t)

    def ag_start(d):
        for s in range(SUB):
            for down in (0, 1):
                pl.when(sends(down, d))(lambda: ag_hop(down, d, s).start())

    def ag_step(d):
        for s in range(SUB):
            for down in (0, 1):

                @pl.when(gets(down, d))
                def _(down=down, s=s):
                    spot = rows_of(origin(down, d), t).at[pl.ds(s * part_rows, part_rows)]
                    remote(
                        spot, spot, ag_sem.at[down, d], ag_land.at[down, d, s], me, 1 - t
                    ).wait_recv()
                    if d < Z - 1:
                        pl.when(sends(down, d + 1))(lambda: ag_hop(down, d + 1, s).start())
                    if s == SUB - 1:
                        to_core(down, d, t).start()

    def ag_done(d):
        for down in (0, 1):

            @pl.when(gets(down, d))
            def _(down=down):
                to_core(down, d, 1 - t).wait_recv()

    def apply(cs, zz, fresh):
        block = all_sc[zz].reshape(T, D)
        lane = 0
        for c in cs:
            n = span_of(c) * LANE
            both = jnp.dot(
                block,
                store(c)[:, :, : 2 * n].reshape(D, 2 * n),
                preferred_element_type=jnp.float32,
            )
            value = jax.nn.silu(both[:, :n]) * both[:, n:]
            hidden[:, lane : lane + n] = value.astype(jnp.bfloat16)
            lane += n
        left = hidden[:, :lane]
        spots = [(c, 2 * span_of(c) + i) for c in cs for i in range(span_of(c))]
        group = 4 if (Z * R) % 8 == 0 else 1

        @pl.loop(0, (Z * R) // (2 * group))
        def _(g):
            for q in range(group):
                p = g * group + q
                right = jnp.concatenate(
                    [
                        jnp.concatenate(
                            [store(c)[2 * p + i, :, k * LANE : (k + 1) * LANE] for c, k in spots],
                            axis=0,
                        )
                        for i in range(2)
                    ],
                    axis=1,
                )
                value = jnp.dot(left, right, preferred_element_type=jnp.float32)
                cols = pl.ds(pl.multiple_of(p * (2 * DN), 2 * DN), 2 * DN)
                if fresh:
                    acc[zz, :, cols] = value
                else:
                    acc[zz, :, cols] = acc[zz, :, cols] + value

    early = tuple(range(pairs))
    late = tuple(range(pairs, chunks))

    def apply_last(cs, zz, fresh):
        cond = here[chunks - 1]
        if cond is None:
            apply(cs, zz, fresh)
            return
        pl.when(cond)(lambda: apply(cs, zz, fresh))
        if cs[:-1]:
            pl.when(jnp.logical_not(cond))(lambda: apply(cs[:-1], zz, fresh))

    def apply_near(cs, d, fresh):
        for down in (0, 1):

            @pl.when(gets(down, d))
            def _(down=down):
                apply(cs, origin(down, d), fresh)

    ag_start(1)
    across = remote(norm_sc, rows_of(z, t), core_sem.at[0, 0], core_sem.at[1, 0], me, 1 - t)
    across.start()
    own = pltpu.make_async_copy(norm_sc, rows_of(z, t), local_sem.at[0])
    own.start()
    first_hop(2, 3)
    for j in range(1, Z):
        first_hop(3, j)
    relay(1, 2)
    spread(2, 1)
    ag_step(1)
    own.wait()
    across.wait_send()
    remote(
        norm_sc, rows_of(z, 1 - t), core_sem.at[0, 0], core_sem.at[1, 0], me, 1 - t
    ).wait_recv()
    spread(2, 2)
    relay(1, 3)
    spread(2, 3)
    for c in early:
        settle(c)
    apply(early, z, True)
    for j in range(1, Z):
        spread(3, j)
    for j in range(1, Z):
        relay(2, j)
    ag_step(2)
    ag_done(1)
    apply_near(early, 1, True)
    for j in range(1, Z):
        relay(3, j)
    ag_done(2)
    apply_near(early, 2, True)
    for c in late:
        settle(c)

    def pick(table):
        spot = jnp.int32(0)
        for zz in range(Z):
            spot = jnp.where(z == zz, table[zz], spot)
        return spot

    goals = [[Z - 2, Z - 1] + list(range(Z - 3, 0, -1)), [1, 0] + list(range(2, Z - 1))]
    ranks = []
    for zz in range(Z):
        seq = [[zd for zd in goal if (zz > zd if down else zz < zd)] for down, goal in enumerate(goals)]
        if zz in (0, Z - 1):
            seq = seq[0] + seq[1]
            seq = [seq[0]] + seq[2:] + [seq[1]]
        else:
            seq = [zd for k in range(Z - 1) for down in (0, 1) for zd in seq[down][k : k + 1]]
        ranks.append(seq + [zz])

    def cross_copy(zz):
        return remote(
            half.at[zz], cross.at[zz], cross_sem.at[0, zz], cross_sem.at[1, zz], me, 1 - t
        )

    other_rows = pl.ds(pl.multiple_of((1 - t) * H, 16), H)
    piece = H // SUB

    def rs_copy(down, k, s):
        rows = pl.ds(s * piece, piece)
        to = z - 1 if down else z + 1
        return remote(
            rs_out.at[down, k, rows],
            rs_in.at[down, k, rows],
            rs_sem.at[down, k],
            rs_land.at[down, k, s],
            dev(to, r),
            t,
        )

    def rs_wait(down, k, s):
        rows = pl.ds(s * piece, piece)
        fro = z + 1 if down else z - 1
        remote(
            rs_out.at[down, k, rows],
            rs_in.at[down, k, rows],
            rs_sem.at[down, k],
            rs_land.at[down, k, s],
            dev(fro, r),
            t,
        ).wait_recv()

    def mine(zd, s):
        rows = pl.ds(s * piece, piece)
        long = pl.ds(pl.multiple_of(t * H + s * piece, 16), piece)
        return acc[zd, long, :] + cross[zd, rows, :].astype(jnp.float32)

    def hand_over(zz):
        half[zz] = acc[zz, other_rows, :].astype(jnp.bfloat16)
        cross_copy(zz).start()

    def rs_step(down, k, inner):
        zd = goals[down][k]
        for s in range(SUB):
            rows = pl.ds(s * piece, piece)
            if s == 0:
                cross_copy(zd).wait_recv()
            total = mine(zd, s)
            if inner:
                rs_wait(down, k, s)
                total = total + rs_in[down, k, rows, :].astype(jnp.float32)
            rs_out[down, k, rows, :] = total.astype(jnp.bfloat16)
            rs_copy(down, k, s).start()

    edge = (z == 0) | (z == Z - 1)

    def edge_step(k):
        pl.when(z == 0)(lambda: rs_step(0, k, False))
        pl.when(z == Z - 1)(lambda: rs_step(1, k, False))

    for n in range(Z):
        zz = pick([ranks[i][n] for i in range(Z)])
        if n == Z - 2:
            for d in range(3, Z):
                ag_step(d)
                ag_done(d)
            pl.when(edge)(lambda: apply_last(early + late, zz, True))
            pl.when(jnp.logical_not(edge))(lambda: apply_last(late, zz, False))
        else:
            apply_last(late, zz, False)
        hand_over(zz)
        if n == 1:
            edge_step(0)
    edge_step(1)
    edge_step(2)
    for half_of, order in ((z < Z // 2, (0, 1)), (z >= Z // 2, (1, 0))):
        for k in range(Z - 1):
            for down in order:
                zd = goals[down][k]
                inner = (z > zd) & (z < Z - 1) if down else (z < zd) & (z > 0)
                pl.when(half_of & inner)(lambda: rs_step(down, k, True))
    cross_copy(z).wait_recv()
    ends = []
    for s in range(SUB):
        rows = pl.ds(s * piece, piece)
        first[rows, :] = first[rows, :] + 0.5 * mine(z, s)
        for down in (0, 1):

            @pl.when(z < Z - 1 if down else z > 0)
            def _(down=down, s=s, rows=rows):
                k = pick([goals[down].index(i) if i in goals[down] else 0 for i in range(Z)])
                rs_wait(down, k, s)
                first[rows, :] = first[rows, :] + 0.5 * rs_in[down, k, rows, :].astype(jnp.float32)

        res[rows, :] = first[rows, :].astype(jnp.bfloat16)
        place = out.at[pl.ds(pl.multiple_of(t * H + s * piece, 16), piece), :]
        c = remote(res.at[rows], place, out_sem.at[0, s], out_sem.at[1, s], me, 1 - t)
        c.start()
        ends.append(c)
        c = pltpu.make_async_copy(res.at[rows], place, local_sem.at[1 + s])
        c.start()
        ends.append(c)
    for c in ends:
        c.wait()
    for zz in range(Z):
        cross_copy(zz).wait_send()
    for d in range(1, Z):
        for down in (0, 1):

            @pl.when(gets(down, d))
            def _(down=down, d=d):
                to_core(down, d, t).wait_send()

            @pl.when(sends(down, d))
            def _(down=down, d=d):
                ag_hop(down, d).wait_send()

    for k in range(Z - 1):
        for down in (0, 1):
            zd = goals[down][k]

            @pl.when(z > zd if down else z < zd)
            def _(down=down, k=k):
                whole = rs_out.at[down, k]
                remote(whole, whole, rs_sem.at[down, k], rs_land.at[down, k, 0], me, 1 - t).wait_send()

    for o in (KV, Q, *range(chunks)):
        first_hops_sent(o)
    for o in (KV, *range(chunks)):
        spread_sent(o)
    for cond, make in started:
        when(cond, lambda make=make: make().wait_send())


def columns_form(
    resid,
    queries,
    keys,
    values,
    lambdas,
    head_gain,
    out_weight,
    norm_gain,
    gate_weight,
    up_weight,
    down_weight,
):
    Z = lambdas.shape[0]
    S = lax.axis_size("sp")
    R = S // Z
    T, D = resid.shape
    H = T // 2
    W = gate_weight.shape[0]
    DN = down_weight.shape[1]
    blocks = gate_weight.shape[1] // LANE
    pairs = blocks // Z // 2
    singles = blocks // Z % 2 + (1 if blocks % Z else 0)
    chunks = pairs + singles
    bf, f32 = jnp.bfloat16, jnp.float32
    vm = pl.BlockSpec(memory_space=pltpu.VMEM)
    hbm = pl.BlockSpec(memory_space=pl.ANY)
    dma = pltpu.SemaphoreType.DMA

    def kernel(*refs):
        whole_kernel(Z, R, blocks, pairs, singles, refs)

    return pl.pallas_call(
        kernel,
        out_shape=jax.ShapeDtypeStruct((T, D), bf),
        in_specs=[hbm] * 8 + [pl.BlockSpec(memory_space=pltpu.SMEM), vm, vm],
        out_specs=vm,
        scratch_shapes=[
            pltpu.VMEM((Z, T, VD), bf),
            pltpu.VMEM((S, T, 2 * VD), bf),
            pltpu.VMEM((pairs, S, W, 6 * LANE), bf),
            pltpu.VMEM((singles, S, W, 3 * LANE), bf),
            pltpu.VMEM((T, D), bf),
            pltpu.VMEM(out_weight.shape, bf),
            pltpu.VMEM((Z, T, VD), bf),
            pltpu.VMEM((Z, T, VD), bf),
            pltpu.VMEM((2, H, D), bf),
            pltpu.VMEM((H, D), bf),
            pltpu.VMEM((H, D), f32),
            pltpu.VMEM((H, D), bf),
            pltpu.VMEM((Z, 2, H, D), bf),
            pltpu.VMEM((T, (2 * pairs + singles) * LANE), bf),
            pltpu.VMEM((Z, T, D), f32),
            pltpu.VMEM((Z, H, D), bf),
            pltpu.VMEM((Z, H, D), bf),
            pltpu.VMEM((2, Z - 1, H, D), bf),
            pltpu.VMEM((2, Z - 1, H, D), bf),
            pltpu.VMEM((H, D), bf),
            dma((chunks + 1 + Z,)),
            dma((chunks + 2, Z - 1)),
            dma((chunks + 1,)),
            dma((chunks + 1, Z, 2)),
            dma((chunks + 1,)),
            dma((chunks + 4,)),
            dma((2, Z)),
            dma((2,)),
            dma((2, Z)),
            dma((2, Z, SUB)),
            dma((2, 2 * Z)),
            dma((2, Z)),
            dma((2, Z - 1)),
            dma((2, Z - 1, SUB)),
            dma((2, SUB)),
        ],
        compiler_params=pltpu.CompilerParams(
            collective_id=0, has_side_effects=True, vmem_limit_bytes=VMEM_LIMIT
        ),
    )(
        queries,
        keys,
        values,
        gate_weight,
        up_weight,
        down_weight,
        resid,
        out_weight,
        lambdas,
        head_gain.reshape(1, -1),
        norm_gain.reshape(1, -1),
    )


def solution(mesh):
    sp, tp = mesh.shape["sp"], mesh.shape["tp"]

    def local(*args):
        heads = args[4].shape[0]
        tok_rows = args[1].shape[0]
        columns = (
            tp == 2
            and heads == 4
            and sp == 4 * heads
            and args[10].shape[1] == LANE
            and args[8].shape[0] == LANE
            and args[8].shape[1] % LANE == 0
            and args[8].shape[1] // LANE // heads == 5
            and args[8].shape[1] // LANE % heads != 0
            and tok_rows % (32 * SUB) == 0
        )
        return (columns_form if columns else generic)(*args)

    return jax.shard_map(
        local,
        mesh=mesh,
        in_specs=(
            P("sp", None),
            P("sp", "tp"),
            P("sp", "tp"),
            P("sp", "tp"),
            P("tp"),
            P(),
            P("tp", None),
            P(),
            P("sp", "tp"),
            P("sp", "tp"),
            P("tp", "sp"),
        ),
        out_specs=P("sp", None),
        check_vma=False,
    )
```

```python
import jax
import jax.numpy as jnp
from jax import lax
from jax.experimental import pallas as pl
from jax.experimental.pallas import tpu as pltpu
from jax.sharding import PartitionSpec as P

QK = 64
VD = 128
LANE = 128
SUB = 3
FINE = 6
VMEM_LIMIT = 60 * 1024 * 1024


def rms_rows(first, norm_gain):
    return (
        first * lax.rsqrt(jnp.mean(first * first, axis=-1, keepdims=True) + 1e-06) * norm_gain
    ).astype(jnp.bfloat16)


def generic(
    resid,
    queries,
    keys,
    values,
    lambdas,
    head_gain,
    out_weight,
    norm_gain,
    gate_weight,
    up_weight,
    down_weight,
):
    tok_rows = queries.shape[0]
    local_heads = lambdas.shape[0]
    model_width = resid.shape[1]
    offset = lax.axis_index("sp") * tok_rows
    query_four = queries.reshape(tok_rows, local_heads, 2, QK)
    score_scale = QK ** (-0.5)
    query_pos = offset + lax.iota(jnp.int32, tok_rows)

    def update(fold_state, key_part, value_part, key_pos):
        run_max, run_sum, run_acc = fold_state
        scores = (
            jnp.einsum("qhcd,khcd->chqk", query_four, key_part, preferred_element_type=jnp.float32)
            * score_scale
        )
        causal_mask = key_pos[None, :] <= query_pos[:, None]
        scores = jnp.where(causal_mask, scores, -1e30)
        new_max = jnp.maximum(run_max, jnp.max(scores, axis=-1))
        expo = jnp.where(causal_mask, jnp.exp(scores - new_max[..., None]), 0.0)
        factor = jnp.exp(run_max - new_max)
        new_sum = run_sum * factor + jnp.sum(expo, axis=-1)
        new_acc = run_acc * factor[..., None] + jnp.einsum(
            "chqk,khd->chqd",
            expo.astype(jnp.bfloat16),
            value_part,
            preferred_element_type=jnp.float32,
        )
        return (new_max, new_sum, new_acc)

    initial = (
        jnp.full((2, local_heads, tok_rows), -1e30, jnp.float32),
        jnp.zeros((2, local_heads, tok_rows), jnp.float32),
        jnp.zeros((2, local_heads, tok_rows, VD), jnp.float32),
    )
    key_rows = lax.all_gather(keys, "sp", axis=0, tiled=True)
    value_rows = lax.all_gather(values, "sp", axis=0, tiled=True)
    key_count = key_rows.shape[0]
    key_span = key_count
    while key_span > 1024 and key_span % 2 == 0:
        key_span = key_span // 2

    def one_span(span_index, inner_state):
        span_start = span_index * key_span
        key_part = lax.dynamic_slice_in_dim(key_rows, span_start, key_span, 0).reshape(
            key_span, local_heads, 2, QK
        )
        value_part = lax.dynamic_slice_in_dim(value_rows, span_start, key_span, 0).reshape(
            key_span, local_heads, VD
        )
        key_pos = span_start + lax.iota(jnp.int32, key_span)
        return update(inner_state, key_part, value_part, key_pos)

    final_max, final_sum, final_acc = lax.fori_loop(0, key_count // key_span, one_span, initial)
    ratio = final_acc / final_sum[..., None]
    mixed_heads = ratio[0] - lambdas[:, None, None] * ratio[1]
    head_out = (
        mixed_heads
        * lax.rsqrt(jnp.mean(mixed_heads * mixed_heads, axis=-1, keepdims=True) + 1e-05)
        * head_gain
    ).astype(jnp.bfloat16)
    out_three = out_weight.reshape(local_heads, VD, model_width)
    own_count = tok_rows // lax.axis_size("tp")
    branch = lax.psum_scatter(
        jnp.einsum("hqd,hde->qe", head_out, out_three, preferred_element_type=jnp.float32).astype(
            jnp.bfloat16
        ),
        "tp",
        scatter_dimension=0,
        tiled=True,
    ).astype(jnp.float32)
    resid_own = lax.dynamic_slice_in_dim(resid, lax.axis_index("tp") * own_count, own_count, 0)
    first = resid_own.astype(jnp.float32) + branch
    normed_all = lax.all_gather(rms_rows(first, norm_gain), "tp", axis=0, tiled=True)
    gate_act = jnp.dot(
        normed_all,
        lax.all_gather(gate_weight, "sp", axis=0, tiled=True),
        preferred_element_type=jnp.float32,
    )
    up_act = jnp.dot(
        normed_all,
        lax.all_gather(up_weight, "sp", axis=0, tiled=True),
        preferred_element_type=jnp.float32,
    )
    hidden = (jax.nn.silu(gate_act) * up_act).astype(jnp.bfloat16)
    terms = jnp.dot(
        hidden,
        lax.all_gather(down_weight, "sp", axis=1, tiled=True),
        preferred_element_type=jnp.float32,
    )
    mixer = lax.psum_scatter(
        terms.astype(jnp.bfloat16), "tp", scatter_dimension=0, tiled=True
    ).astype(jnp.float32)
    finished = (first + 0.5 * mixer).astype(jnp.bfloat16)
    return lax.all_gather(finished, "tp", axis=0, tiled=True)


def where_am_i(R):
    s = lax.axis_index("sp")
    return s // R, lax.rem(s, R), lax.axis_index("tp")


def remote(src, dst, send, recv, sp, tp):
    return pltpu.make_async_remote_copy(
        src_ref=src,
        dst_ref=dst,
        send_sem=send,
        recv_sem=recv,
        device_id={"sp": sp, "tp": tp},
        device_id_type=pl.DeviceIdType.MESH,
    )


def greet(peers):
    barrier = pltpu.get_barrier_semaphore()
    for sp, tp in peers:
        pl.semaphore_signal(
            barrier,
            inc=1,
            device_id={"sp": sp, "tp": tp},
            device_id_type=pl.DeviceIdType.MESH,
        )
    pl.semaphore_wait(barrier, len(peers))


def mirror_x(r):
    return r + 1 - 2 * lax.rem(r, 2)


def mirror_y(r):
    return r + 2 - 4 * (lax.rem(r, 4) // 2)


def attention_block(R, T, i, r, q_at, k_at, v_at, lam, gain):
    span = R * T
    query = q_at(i) * jnp.bfloat16(QK**-0.5)
    ratios = []
    for c in range(2):
        part = query[:, c * QK : (c + 1) * QK]

        def fold(n, state, masked):
            run_max, run_sum, run_acc = state
            key = k_at(n)[:, c * QK : (c + 1) * QK]
            scores = lax.dot_general(
                part, key, (((1,), (1,)), ((), ())), preferred_element_type=jnp.float32
            )
            if masked:
                qpos = r * T + lax.broadcasted_iota(jnp.int32, scores.shape, 0)
                kpos = lax.broadcasted_iota(jnp.int32, scores.shape, 1)
                scores = jnp.where(kpos <= qpos, scores, -1e30)
            new_max = jnp.maximum(run_max, jnp.max(scores, axis=-1, keepdims=True))
            expo = jnp.exp(scores - new_max)
            factor = jnp.exp(run_max - new_max)
            new_sum = run_sum * factor + jnp.sum(expo, axis=-1, keepdims=True)
            new_acc = run_acc * factor + jnp.dot(
                expo.astype(jnp.bfloat16), v_at(n), preferred_element_type=jnp.float32
            )
            return new_max, new_sum, new_acc

        state = (
            jnp.full((T, 1), -1e30, jnp.float32),
            jnp.zeros((T, 1), jnp.float32),
            jnp.zeros((T, VD), jnp.float32),
        )
        state = fold(i, state, True)
        state = lax.fori_loop(0, i, lambda n, st: fold(n, st, False), state)
        ratios.append(state[2] / state[1])
    mixed = ratios[0] - lam * ratios[1]
    return (
        mixed * lax.rsqrt(jnp.mean(mixed * mixed, axis=-1, keepdims=True) + 1e-05) * gain
    ).astype(jnp.bfloat16)


def block_start(blocks, Z, zz):
    extra = blocks % Z
    return blocks // Z * zz + jnp.minimum(jnp.maximum(zz - (Z - extra) // 2, 0), extra)


def when(cond, body):
    if cond is None:
        body()
    else:
        pl.when(cond)(body)


def whole_kernel(Z, R, blocks, pairs, singles, refs):
    (
        q_in, k_in, v_in, g_in, u_in, d_in, resid_in, w_in, lam, head_gain, norm_gain,
        out,
        q_sc, kv_sc, wide_sc, thin_sc, resid, w,
        ho, heads, part, got, first, norm_sc, all_sc,
        hidden, acc, half, cross, rs_out, rs_in, res,
        zs, zr, ps, pr, pl_sem, local_sem, ho_sem, swap_sem, ag_sem, ag_land, core_sem,
        cross_sem, rs_sem, rs_land, out_sem,
    ) = refs
    z, r, t = where_am_i(R)
    me = z * R + r
    rx, ry = mirror_x(r), mirror_y(r)
    rd = mirror_x(ry)
    T = k_in.shape[0]
    D = resid_in.shape[1]
    DN = d_in.shape[1]
    H = T // 2
    ahead = [lax.rem(z + j, Z) for j in range(Z)]
    behind = [lax.rem(z + Z - j, Z) for j in range(Z)]
    chunks = pairs + singles
    uneven = blocks % Z != 0
    Q, KV = chunks, chunks + 1

    def dev(zz, rr):
        return zz * R + rr

    def span_of(c):
        return 2 if c < pairs else 1

    def offset(c):
        return 2 * c if c < pairs else pairs + c

    def store(o):
        if o == Q:
            return q_sc
        if o == KV:
            return kv_sc
        return wide_sc.at[o] if o < pairs else thin_sc.at[o - pairs]

    def present(o, zz):
        if not uneven or o != chunks - 1:
            return None
        count = block_start(blocks, Z, zz + 1) - block_start(blocks, Z, zz)
        return count > blocks // Z

    here = [present(o, z) for o in range(chunks + 2)]

    def parts(o, zz, slot):
        if o >= chunks:
            cols = pl.ds(pl.multiple_of(zz * VD, LANE), VD)
            if o == Q:
                return [(q_in.at[:, cols], q_sc.at[slot])]
            return [
                (ref.at[:, cols], kv_sc.at[slot, :, pl.ds(i * VD, VD)])
                for i, ref in enumerate((k_in, v_in))
            ]
        n = span_of(o)
        dst = store(o)
        start = pl.multiple_of((block_start(blocks, Z, zz) + offset(o)) * LANE, LANE)
        pairs_ = [
            (ref.at[:, pl.ds(start, n * LANE)], dst.at[slot, :, pl.ds(i * n * LANE, n * LANE)])
            for i, ref in enumerate((g_in, u_in))
        ]
        for i in range(n):
            rows = pl.ds(pl.multiple_of(start + i * LANE, LANE), LANE)
            pairs_.append((d_in.at[rows, :], dst.at[slot, :, pl.ds((2 * n + i) * LANE, LANE)]))
        return pairs_

    def slot_of(o, zz):
        return zz if o == Q else dev(zz, r)

    def zsend(o, j):
        return zs.at[o if here[o] is None else chunks + 1 + j]

    def first_hop(o, j):
        def body():
            for src, dst in parts(o, ahead[j], slot_of(o, z)):
                remote(src, dst, zsend(o, j), zr.at[o, j - 1], dev(ahead[j], r), t).start()

        when(present(o, ahead[j]), body)

    def arrived(o, j):
        spot = store(o).at[slot_of(o, behind[j])]

        def body():
            remote(spot, spot, zsend(o, j), zr.at[o, j - 1], dev(behind[j], r), t).wait_recv()

        when(here[o], body)

    def first_hops_sent(o):
        if here[o] is None:
            whole = store(o).at[pl.ds(0, Z - 1)]
            remote(whole, whole, zsend(o, 1), zr.at[o, 0], dev(ahead[1], r), t).wait_send()
            return
        for j in range(1, Z):
            spot = store(o).at[0]
            when(
                present(o, ahead[j]),
                lambda j=j: remote(
                    spot, spot, zsend(o, j), zr.at[o, j - 1], dev(ahead[j], r), t
                ).wait_send(),
            )

    def keep(o):
        def body():
            for src, dst in parts(o, z, slot_of(o, z)):
                pltpu.make_async_copy(src, dst, local_sem.at[o]).start()

        when(here[o], body)

    def kept(o):
        spot = store(o).at[slot_of(o, z)]
        when(here[o], lambda: pltpu.make_async_copy(spot, spot, local_sem.at[o]).wait())

    def piece(o, j, owner, h):
        ref = store(o)
        n = ref.shape[1] // 2
        return ref.at[dev(behind[j], owner), pl.ds(h * n, n), :]

    def psem(o):
        return o if o < chunks else chunks

    def landing(o, j, kind):
        p = psem(o)
        return pr.at[p, j] if kind in (0, 3) else pl_sem.at[p]

    def hop2(o, j, kind):
        owner = (r, r, r, r, rx, ry)[kind]
        target = (rx, rx, ry, ry, ry, rx)[kind]
        spot = piece(o, j, owner, kind % 2)
        return remote(spot, spot, ps.at[psem(o)], landing(o, j, kind), dev(z, target), t)

    def wait2(o, j):
        spot = store(o).at[dev(behind[j], rx)]
        remote(spot, spot, ps.at[psem(o)], landing(o, j, 0), dev(z, rx), t).wait_recv()

    def spread(o, j):
        if j:
            arrived(o, j)
        else:
            kept(o)

        def body():
            for kind in (0, 3, 1, 2):
                hop2(o, j, kind).start()

        when(here[o], body)

    def relay(o, j):
        def body():
            wait2(o, j)
            hop2(o, j, 4).start()
            hop2(o, j, 5).start()

        when(here[o], body)

    def settle(o):
        whole = store(o).at[pl.ds(0, 2 * Z)]
        when(
            here[o],
            lambda: remote(
                whole, whole, ps.at[psem(o)], landing(o, 0, 1), dev(z, rx), t
            ).wait_recv(),
        )

    def spread_sent(o):
        whole = store(o).at[pl.ds(0, 3 * Z)]
        when(
            here[o],
            lambda: remote(
                whole, whole, ps.at[psem(o)], landing(o, 0, 1), dev(z, rx), t
            ).wait_send(),
        )

    for o in (KV, *range(chunks), Q):
        keep(o)
    resid_copy = pltpu.make_async_copy(resid_in, resid, local_sem.at[chunks + 2])
    resid_copy.start()
    w_copy = pltpu.make_async_copy(w_in, w, local_sem.at[chunks + 3])
    w_copy.start()

    greet(
        [(dev(ahead[j], r), t) for j in range(1, Z)]
        + [(dev(z, rx), t), (dev(z, ry), t), (me, 1 - t)]
    )
    for o in (KV, Q, 0, 1):
        for j in range(1, Z):
            first_hop(o, j)
        if o == KV:
            spread(KV, 0)
    spread(0, 0)
    relay(KV, 0)
    for j in range(1, Z):
        spread(KV, j)
        if j > 1:
            relay(KV, j - 1)
        if j == Z - 2:
            spread(1, 0)
    relay(0, 0)
    relay(KV, Z - 1)
    for c in range(2, chunks):
        spread(c, 0)
    settle(KV)
    kept(Q)
    for j in range(1, Z):
        arrived(Q, j)

    head_lam = lam[z]

    def span(n, first_lane):
        return kv_sc[pl.ds(n * R, R), :, first_lane : first_lane + VD].reshape(R * T, VD)

    def ho_copy(i):
        return remote(ho.at[i], heads.at[z], ho_sem.at[Z], ho_sem.at[z], dev(i, r), t)

    for i in range(Z):
        ho[i] = attention_block(
            R, T, i, r,
            lambda b: q_sc[b],
            lambda n: span(n, 0),
            lambda n: span(n, VD),
            head_lam,
            head_gain[...],
        )

        @pl.when(z == i)
        def _(i=i):
            heads[i] = ho[i]

        pl.when(z != i)(lambda i=i: ho_copy(i).start())
        if i == 0:
            relay(1, 0)
            spread(0, 1)
        if i == 1:
            relay(2, 0)
            relay(3, 0)
        if i == 2:
            spread(0, 2)
            relay(0, 1)
    spread(0, 3)
    relay(0, 2)
    spread(1, 1)
    spread(1, 2)
    relay(0, 3)
    spread(1, 3)
    relay(1, 1)
    resid_copy.wait()
    w_copy.wait()
    for i in range(Z):

        @pl.when(z != i)
        def _(i=i):
            remote(
                ho.at[i], heads.at[i], ho_sem.at[Z], ho_sem.at[i], dev(i, r), t
            ).wait_recv()

    first_hop(2, 1)
    first_hop(2, 2)
    NT = 512 if D % 512 == 0 else D
    for h in range(2):
        hh = (1 - t) if h == 0 else t
        rows = pl.ds(pl.multiple_of(hh * H, 16), H)
        left = jnp.concatenate([heads[n, rows, :] for n in range(Z)], axis=1)
        for n in range(0, D, NT):
            part[h, :, n : n + NT] = jnp.dot(
                left, w[:, n : n + NT], preferred_element_type=jnp.float32
            ).astype(jnp.bfloat16)
        if h == 0:
            swap = remote(part.at[0], got, swap_sem.at[0], swap_sem.at[1], me, 1 - t)
            swap.start()
    swap.wait()
    own_rows = pl.ds(pl.multiple_of(t * H, 16), H)
    first_val = resid[own_rows, :].astype(jnp.float32) + (
        part[1].astype(jnp.float32) + got[...].astype(jnp.float32)
    )
    first[...] = first_val
    norm_sc[...] = rms_rows(first_val, norm_gain[...])

    def rows_of(zz, tt):
        return all_sc.at[zz, tt]

    part_rows = H // SUB

    def ag_hop(down, d, s=None):
        zz = z + (d - 1) if down else z - (d - 1)
        to = z - 1 if down else z + 1
        src = norm_sc if d == 1 else rows_of(zz, t)
        dst = rows_of(zz, t)
        if s is not None:
            src, dst = (ref.at[pl.ds(s * part_rows, part_rows)] for ref in (src, dst))
        return remote(
            src, dst, ag_sem.at[down, d], ag_land.at[down, d, 0 if s is None else s], dev(to, r), t
        )

    def sends(down, d):
        return (z > 0) & (z + (d - 1) < Z) if down else (z + 1 < Z) & (z - (d - 1) >= 0)

    def gets(down, d):
        return z + d < Z if down else z - d >= 0

    def origin(down, d):
        return z + d if down else z - d

    def to_core(down, d, tt):
        rows = rows_of(origin(down, d), tt)
        n = 2 * d + down
        return remote(rows, rows, core_sem.at[2 * Z], core_sem.at[n], me, 1 - t)

    def ag_start(d):
        for s in range(SUB):
            for down in (0, 1):
                pl.when(sends(down, d))(lambda: ag_hop(down, d, s).start())

    def ag_step(d):
        for s in range(SUB):
            for down in (0, 1):

                @pl.when(gets(down, d))
                def _(down=down, s=s):
                    spot = rows_of(origin(down, d), t).at[pl.ds(s * part_rows, part_rows)]
                    remote(
                        spot, spot, ag_sem.at[down, d], ag_land.at[down, d, s], me, 1 - t
                    ).wait_recv()
                    if d < Z - 1:
                        pl.when(sends(down, d + 1))(lambda: ag_hop(down, d + 1, s).start())
                    if s == SUB - 1:
                        to_core(down, d, t).start()

    def ag_done(d):
        for down in (0, 1):

            @pl.when(gets(down, d))
            def _(down=down):
                to_core(down, d, 1 - t).wait_recv()

    def apply(cs, zz, fresh):
        block = all_sc[zz].reshape(T, D)
        lane = 0
        for c in cs:
            n = span_of(c) * LANE
            both = jnp.dot(
                block,
                store(c)[:, :, : 2 * n].reshape(D, 2 * n),
                preferred_element_type=jnp.float32,
            )
            value = jax.nn.silu(both[:, :n]) * both[:, n:]
            hidden[:, lane : lane + n] = value.astype(jnp.bfloat16)
            lane += n
        left = hidden[:, :lane]
        spots = [(c, 2 * span_of(c) + i) for c in cs for i in range(span_of(c))]
        group = 4 if (Z * R) % 8 == 0 else 1

        @pl.loop(0, (Z * R) // (2 * group))
        def _(g):
            for q in range(group):
                p = g * group + q
                right = jnp.concatenate(
                    [
                        jnp.concatenate(
                            [store(c)[2 * p + i, :, k * LANE : (k + 1) * LANE] for c, k in spots],
                            axis=0,
                        )
                        for i in range(2)
                    ],
                    axis=1,
                )
                value = jnp.dot(left, right, preferred_element_type=jnp.float32)
                cols = pl.ds(pl.multiple_of(p * (2 * DN), 2 * DN), 2 * DN)
                if fresh:
                    acc[zz, :, cols] = value
                else:
                    acc[zz, :, cols] = acc[zz, :, cols] + value

    early = tuple(range(pairs))
    late = tuple(range(pairs, chunks))

    def apply_last(cs, zz, fresh):
        cond = here[chunks - 1]
        if cond is None:
            apply(cs, zz, fresh)
            return
        pl.when(cond)(lambda: apply(cs, zz, fresh))
        if cs[:-1]:
            pl.when(jnp.logical_not(cond))(lambda: apply(cs[:-1], zz, fresh))

    def apply_near(cs, d, fresh):
        for down in (0, 1):

            @pl.when(gets(down, d))
            def _(down=down):
                apply(cs, origin(down, d), fresh)

    ag_start(1)
    across = remote(norm_sc, rows_of(z, t), core_sem.at[2 * Z], core_sem.at[0], me, 1 - t)
    across.start()
    own = pltpu.make_async_copy(norm_sc, rows_of(z, t), local_sem.at[0])
    own.start()
    first_hop(2, 3)
    for j in range(1, Z):
        first_hop(3, j)
    relay(1, 2)
    spread(2, 1)
    spread(2, 2)
    relay(1, 3)
    settle(0)
    own.wait()
    remote(
        norm_sc, rows_of(z, 1 - t), core_sem.at[2 * Z], core_sem.at[0], me, 1 - t
    ).wait_recv()
    apply((0,), z, True)
    ag_step(1)
    spread(2, 3)
    relay(2, 1)
    ag_done(1)
    apply_near((0,), 1, True)
    settle(1)
    apply((1,), z, False)
    for j in range(1, Z):
        spread(3, j)
    relay(2, 2)
    relay(2, 3)
    apply_near((1,), 1, False)
    ag_step(2)
    relay(3, 1)
    relay(3, 2)
    relay(3, 3)
    ag_done(2)
    apply_near(early, 2, True)
    for c in late:
        settle(c)

    def pick(table):
        spot = jnp.int32(0)
        for zz in range(Z):
            spot = jnp.where(z == zz, table[zz], spot)
        return spot

    goals = [[Z - 2, Z - 1] + list(range(Z - 3, 0, -1)), [1, 0] + list(range(2, Z - 1))]
    ranks = []
    for zz in range(Z):
        seq = [[zd for zd in goal if (zz > zd if down else zz < zd)] for down, goal in enumerate(goals)]
        if zz in (0, Z - 1):
            seq = seq[0] + seq[1]
            ranks.append([seq[0]] + seq[2:] + [zz, seq[1]])
        else:
            seq = [zd for k in range(Z - 1) for down in (0, 1) for zd in seq[down][k : k + 1]]
            ranks.append(seq + [zz])

    def cross_copy(zz):
        return remote(
            half.at[zz], cross.at[zz], cross_sem.at[Z], cross_sem.at[zz], me, 1 - t
        )

    other_rows = pl.ds(pl.multiple_of((1 - t) * H, 16), H)
    small = H // FINE

    def rs_copy(down, k, s):
        rows = pl.ds(s * small, small)
        to = z - 1 if down else z + 1
        return remote(
            rs_out.at[down, k, rows],
            rs_in.at[down, k, rows],
            rs_sem.at[down, k],
            rs_land.at[down, k, s],
            dev(to, r),
            t,
        )

    def rs_wait(down, k, s):
        rows = pl.ds(s * small, small)
        fro = z + 1 if down else z - 1
        remote(
            rs_out.at[down, k, rows],
            rs_in.at[down, k, rows],
            rs_sem.at[down, k],
            rs_land.at[down, k, s],
            dev(fro, r),
            t,
        ).wait_recv()

    def mine(zd, s):
        rows = pl.ds(s * small, small)
        long = pl.ds(pl.multiple_of(t * H + s * small, 16), small)
        return acc[zd, long, :] + cross[zd, rows, :].astype(jnp.float32)

    def hand_over(zz):
        half[zz] = acc[zz, other_rows, :].astype(jnp.bfloat16)
        cross_copy(zz).start()

    def rs_step(down, k, inner, subs=range(FINE)):
        zd = goals[down][k]
        for s in subs:
            rows = pl.ds(s * small, small)
            if s == 0:
                cross_copy(zd).wait_recv()
            total = mine(zd, s)
            if inner:
                rs_wait(down, k, s)
                total = total + rs_in[down, k, rows, :].astype(jnp.float32)
            rs_out[down, k, rows, :] = total.astype(jnp.bfloat16)
            rs_copy(down, k, s).start()

    edge = (z == 0) | (z == Z - 1)

    def edge_step(k, low=(0, FINE), high=(0, FINE)):
        pl.when(z == 0)(lambda: rs_step(0, k, False, range(*low)))
        pl.when(z == Z - 1)(lambda: rs_step(1, k, False, range(*high)))

    def inner_step(k, subs=range(FINE), lag=0):
        for half_of, order in ((z < Z // 2, (0, 1)), (z >= Z // 2, (1, 0))):
            for s in range(subs[0], subs[-1] + 1 + lag):
                for down, at in zip(order, (s, s - lag)):
                    if at not in subs:
                        continue
                    zd = goals[down][k]
                    inner = (z > zd) & (z < Z - 1) if down else (z < zd) & (z > 0)
                    pl.when(half_of & inner)(lambda: rs_step(down, k, True, (at,)))

    for n in range(Z):
        zz = pick([ranks[i][n] for i in range(Z)])
        if n == Z - 1:
            for d in range(3, Z):
                ag_step(d)
                ag_done(d)
            pl.when(edge)(lambda: apply_last(early + late, zz, True))
            pl.when(jnp.logical_not(edge))(lambda: apply_last(late, zz, False))
        else:
            apply_last(late, zz, False)
        hand_over(zz)
        if n == 1:
            edge_step(0)
            edge_step(2, (0, 2), (0, 1))
            inner_step(0, range(FINE // 3))
        if n == 2:
            inner_step(0, range(FINE // 3, 2 * FINE // 3))
    edge_step(1)
    edge_step(2, (2, FINE), (1, FINE))
    inner_step(0, range(2 * FINE // 3, FINE))
    for k in range(1, Z - 1):
        inner_step(k, range(FINE), 2)
    cross_copy(z).wait_recv()
    for s in range(FINE):
        rows = pl.ds(s * small, small)
        first[rows, :] = first[rows, :] + 0.5 * mine(z, s)
        for down in (0, 1):

            @pl.when(z < Z - 1 if down else z > 0)
            def _(down=down, s=s, rows=rows):
                k = pick([goals[down].index(i) if i in goals[down] else 0 for i in range(Z)])
                rs_wait(down, k, s)
                first[rows, :] = first[rows, :] + 0.5 * rs_in[down, k, rows, :].astype(jnp.float32)

        res[rows, :] = first[rows, :].astype(jnp.bfloat16)
        place = out.at[pl.ds(pl.multiple_of(t * H + s * small, 16), small), :]
        remote(res.at[rows], place, out_sem.at[0], out_sem.at[1], me, 1 - t).start()
        pltpu.make_async_copy(res.at[rows], place, local_sem.at[1]).start()
    theirs = out.at[pl.ds(pl.multiple_of((1 - t) * H, 16), H), :]
    remote(res, theirs, out_sem.at[0], out_sem.at[1], me, 1 - t).wait()
    pltpu.make_async_copy(res, out.at[own_rows, :], local_sem.at[1]).wait()
    remote(half, cross, cross_sem.at[Z], cross_sem.at[0], me, 1 - t).wait_send()
    remote(half, cross, core_sem.at[2 * Z], core_sem.at[0], me, 1 - t).wait_send()
    for d in range(1, Z):
        for down in (0, 1):

            @pl.when(sends(down, d))
            def _(down=down, d=d):
                ag_hop(down, d).wait_send()

    for k in range(Z - 1):
        for down in (0, 1):
            zd = goals[down][k]

            @pl.when(z > zd if down else z < zd)
            def _(down=down, k=k):
                whole = rs_out.at[down, k]
                remote(whole, whole, rs_sem.at[down, k], rs_land.at[down, k, 0], me, 1 - t).wait_send()

    for o in (KV, Q, *range(chunks)):
        first_hops_sent(o)
    for o in (KV, *range(chunks)):
        spread_sent(o)
    sent = ho.at[pl.ds(0, Z - 1)]
    remote(sent, sent, ho_sem.at[Z], ho_sem.at[0], me, 1 - t).wait_send()


def columns_form(
    resid,
    queries,
    keys,
    values,
    lambdas,
    head_gain,
    out_weight,
    norm_gain,
    gate_weight,
    up_weight,
    down_weight,
):
    Z = lambdas.shape[0]
    S = lax.axis_size("sp")
    R = S // Z
    T, D = resid.shape
    H = T // 2
    W = gate_weight.shape[0]
    DN = down_weight.shape[1]
    blocks = gate_weight.shape[1] // LANE
    pairs = blocks // Z // 2
    singles = blocks // Z % 2 + (1 if blocks % Z else 0)
    chunks = pairs + singles
    bf, f32 = jnp.bfloat16, jnp.float32
    vm = pl.BlockSpec(memory_space=pltpu.VMEM)
    hbm = pl.BlockSpec(memory_space=pl.ANY)
    dma = pltpu.SemaphoreType.DMA

    def kernel(*refs):
        whole_kernel(Z, R, blocks, pairs, singles, refs)

    return pl.pallas_call(
        kernel,
        out_shape=pltpu.VMEM((T, D), bf),
        in_specs=[hbm] * 8 + [pl.BlockSpec(memory_space=pltpu.SMEM), vm, vm],
        out_specs=vm,
        scratch_shapes=[
            pltpu.VMEM((Z, T, VD), bf),
            pltpu.VMEM((S, T, 2 * VD), bf),
            pltpu.VMEM((pairs, S, W, 6 * LANE), bf),
            pltpu.VMEM((singles, S, W, 3 * LANE), bf),
            pltpu.VMEM((T, D), bf),
            pltpu.VMEM(out_weight.shape, bf),
            pltpu.VMEM((Z, T, VD), bf),
            pltpu.VMEM((Z, T, VD), bf),
            pltpu.VMEM((2, H, D), bf),
            pltpu.VMEM((H, D), bf),
            pltpu.VMEM((H, D), f32),
            pltpu.VMEM((H, D), bf),
            pltpu.VMEM((Z, 2, H, D), bf),
            pltpu.VMEM((T, (2 * pairs + singles) * LANE), bf),
            pltpu.VMEM((Z, T, D), f32),
            pltpu.VMEM((Z, H, D), bf),
            pltpu.VMEM((Z, H, D), bf),
            pltpu.VMEM((2, Z - 1, H, D), bf),
            pltpu.VMEM((2, Z - 1, H, D), bf),
            pltpu.VMEM((H, D), bf),
            dma((chunks + 1 + Z,)),
            dma((chunks + 2, Z - 1)),
            dma((chunks + 1,)),
            dma((chunks + 1, Z)),
            dma((chunks + 1,)),
            dma((chunks + 4,)),
            dma((Z + 1,)),
            dma((2,)),
            dma((2, Z)),
            dma((2, Z, SUB)),
            dma((2 * Z + 1,)),
            dma((Z + 1,)),
            dma((2, Z - 1)),
            dma((2, Z - 1, FINE)),
            dma((2,)),
        ],
        compiler_params=pltpu.CompilerParams(
            collective_id=0, has_side_effects=True, vmem_limit_bytes=VMEM_LIMIT
        ),
    )(
        queries,
        keys,
        values,
        gate_weight,
        up_weight,
        down_weight,
        resid,
        out_weight,
        lambdas,
        head_gain.reshape(1, -1),
        norm_gain.reshape(1, -1),
    )


def solution(mesh):
    sp, tp = mesh.shape["sp"], mesh.shape["tp"]

    def local(*args):
        heads = args[4].shape[0]
        tok_rows = args[1].shape[0]
        columns = (
            tp == 2
            and heads == 4
            and sp == 4 * heads
            and args[10].shape[1] == LANE
            and args[8].shape[0] == LANE
            and args[8].shape[1] % LANE == 0
            and args[8].shape[1] // LANE // heads == 5
            and args[8].shape[1] // LANE % heads != 0
            and tok_rows % (32 * FINE) == 0
            and FINE % SUB == 0
        )
        return (columns_form if columns else generic)(*args)

    return jax.shard_map(
        local,
        mesh=mesh,
        in_specs=(
            P("sp", None),
            P("sp", "tp"),
            P("sp", "tp"),
            P("sp", "tp"),
            P("tp"),
            P(),
            P("tp", None),
            P(),
            P("sp", "tp"),
            P("sp", "tp"),
            P("tp", "sp"),
        ),
        out_specs=P("sp", None),
        check_vma=False,
    )
```

```python
import jax
import jax.numpy as jnp
from jax import lax
from jax.experimental import pallas as pl
from jax.experimental.pallas import tpu as pltpu
from jax.sharding import PartitionSpec as P

QK = 64
VD = 128
LANE = 128
SUB = 3
FINE = 6
VMEM_LIMIT = 60 * 1024 * 1024


def rms_rows(first, norm_gain):
    return (
        first * lax.rsqrt(jnp.mean(first * first, axis=-1, keepdims=True) + 1e-06) * norm_gain
    ).astype(jnp.bfloat16)


def generic(
    resid,
    queries,
    keys,
    values,
    lambdas,
    head_gain,
    out_weight,
    norm_gain,
    gate_weight,
    up_weight,
    down_weight,
):
    tok_rows = queries.shape[0]
    local_heads = lambdas.shape[0]
    model_width = resid.shape[1]
    offset = lax.axis_index("sp") * tok_rows
    query_four = queries.reshape(tok_rows, local_heads, 2, QK)
    score_scale = QK ** (-0.5)
    query_pos = offset + lax.iota(jnp.int32, tok_rows)

    def update(fold_state, key_part, value_part, key_pos):
        run_max, run_sum, run_acc = fold_state
        scores = (
            jnp.einsum("qhcd,khcd->chqk", query_four, key_part, preferred_element_type=jnp.float32)
            * score_scale
        )
        causal_mask = key_pos[None, :] <= query_pos[:, None]
        scores = jnp.where(causal_mask, scores, -1e30)
        new_max = jnp.maximum(run_max, jnp.max(scores, axis=-1))
        expo = jnp.where(causal_mask, jnp.exp(scores - new_max[..., None]), 0.0)
        factor = jnp.exp(run_max - new_max)
        new_sum = run_sum * factor + jnp.sum(expo, axis=-1)
        new_acc = run_acc * factor[..., None] + jnp.einsum(
            "chqk,khd->chqd",
            expo.astype(jnp.bfloat16),
            value_part,
            preferred_element_type=jnp.float32,
        )
        return (new_max, new_sum, new_acc)

    initial = (
        jnp.full((2, local_heads, tok_rows), -1e30, jnp.float32),
        jnp.zeros((2, local_heads, tok_rows), jnp.float32),
        jnp.zeros((2, local_heads, tok_rows, VD), jnp.float32),
    )
    key_rows = lax.all_gather(keys, "sp", axis=0, tiled=True)
    value_rows = lax.all_gather(values, "sp", axis=0, tiled=True)
    key_count = key_rows.shape[0]
    key_span = key_count
    while key_span > 1024 and key_span % 2 == 0:
        key_span = key_span // 2

    def one_span(span_index, inner_state):
        span_start = span_index * key_span
        key_part = lax.dynamic_slice_in_dim(key_rows, span_start, key_span, 0).reshape(
            key_span, local_heads, 2, QK
        )
        value_part = lax.dynamic_slice_in_dim(value_rows, span_start, key_span, 0).reshape(
            key_span, local_heads, VD
        )
        key_pos = span_start + lax.iota(jnp.int32, key_span)
        return update(inner_state, key_part, value_part, key_pos)

    final_max, final_sum, final_acc = lax.fori_loop(0, key_count // key_span, one_span, initial)
    ratio = final_acc / final_sum[..., None]
    mixed_heads = ratio[0] - lambdas[:, None, None] * ratio[1]
    head_out = (
        mixed_heads
        * lax.rsqrt(jnp.mean(mixed_heads * mixed_heads, axis=-1, keepdims=True) + 1e-05)
        * head_gain
    ).astype(jnp.bfloat16)
    out_three = out_weight.reshape(local_heads, VD, model_width)
    own_count = tok_rows // lax.axis_size("tp")
    branch = lax.psum_scatter(
        jnp.einsum("hqd,hde->qe", head_out, out_three, preferred_element_type=jnp.float32).astype(
            jnp.bfloat16
        ),
        "tp",
        scatter_dimension=0,
        tiled=True,
    ).astype(jnp.float32)
    resid_own = lax.dynamic_slice_in_dim(resid, lax.axis_index("tp") * own_count, own_count, 0)
    first = resid_own.astype(jnp.float32) + branch
    normed_all = lax.all_gather(rms_rows(first, norm_gain), "tp", axis=0, tiled=True)
    gate_act = jnp.dot(
        normed_all,
        lax.all_gather(gate_weight, "sp", axis=0, tiled=True),
        preferred_element_type=jnp.float32,
    )
    up_act = jnp.dot(
        normed_all,
        lax.all_gather(up_weight, "sp", axis=0, tiled=True),
        preferred_element_type=jnp.float32,
    )
    hidden = (jax.nn.silu(gate_act) * up_act).astype(jnp.bfloat16)
    terms = jnp.dot(
        hidden,
        lax.all_gather(down_weight, "sp", axis=1, tiled=True),
        preferred_element_type=jnp.float32,
    )
    mixer = lax.psum_scatter(
        terms.astype(jnp.bfloat16), "tp", scatter_dimension=0, tiled=True
    ).astype(jnp.float32)
    finished = (first + 0.5 * mixer).astype(jnp.bfloat16)
    return lax.all_gather(finished, "tp", axis=0, tiled=True)


def where_am_i(R):
    s = lax.axis_index("sp")
    return s // R, lax.rem(s, R), lax.axis_index("tp")


def remote(src, dst, send, recv, sp, tp):
    return pltpu.make_async_remote_copy(
        src_ref=src,
        dst_ref=dst,
        send_sem=send,
        recv_sem=recv,
        device_id={"sp": sp, "tp": tp},
        device_id_type=pl.DeviceIdType.MESH,
    )


def greet(peers):
    barrier = pltpu.get_barrier_semaphore()
    for sp, tp in peers:
        pl.semaphore_signal(
            barrier,
            inc=1,
            device_id={"sp": sp, "tp": tp},
            device_id_type=pl.DeviceIdType.MESH,
        )
    pl.semaphore_wait(barrier, len(peers))


def mirror_x(r):
    return r + 1 - 2 * lax.rem(r, 2)


def mirror_y(r):
    return r + 2 - 4 * (lax.rem(r, 4) // 2)


def attention_block(R, T, i, r, q_at, k_at, v_at, lam, gain):
    span = R * T
    query = q_at(i) * jnp.bfloat16(QK**-0.5)
    ratios = []
    for c in range(2):
        part = query[:, c * QK : (c + 1) * QK]

        def fold(n, state, masked):
            run_max, run_sum, run_acc = state
            key = k_at(n)[:, c * QK : (c + 1) * QK]
            scores = lax.dot_general(
                part, key, (((1,), (1,)), ((), ())), preferred_element_type=jnp.float32
            )
            if masked:
                qpos = r * T + lax.broadcasted_iota(jnp.int32, scores.shape, 0)
                kpos = lax.broadcasted_iota(jnp.int32, scores.shape, 1)
                scores = jnp.where(kpos <= qpos, scores, -1e30)
            new_max = jnp.maximum(run_max, jnp.max(scores, axis=-1, keepdims=True))
            expo = jnp.exp(scores - new_max)
            factor = jnp.exp(run_max - new_max)
            new_sum = run_sum * factor + jnp.sum(expo, axis=-1, keepdims=True)
            new_acc = run_acc * factor + jnp.dot(
                expo.astype(jnp.bfloat16), v_at(n), preferred_element_type=jnp.float32
            )
            return new_max, new_sum, new_acc

        state = (
            jnp.full((T, 1), -1e30, jnp.float32),
            jnp.zeros((T, 1), jnp.float32),
            jnp.zeros((T, VD), jnp.float32),
        )
        state = fold(i, state, True)
        state = lax.fori_loop(0, i, lambda n, st: fold(n, st, False), state)
        ratios.append(state[2] / state[1])
    mixed = ratios[0] - lam * ratios[1]
    return (
        mixed * lax.rsqrt(jnp.mean(mixed * mixed, axis=-1, keepdims=True) + 1e-05) * gain
    ).astype(jnp.bfloat16)


def block_start(blocks, Z, zz):
    extra = blocks % Z
    return blocks // Z * zz + jnp.minimum(jnp.maximum(zz - (Z - extra) // 2, 0), extra)


def when(cond, body):
    if cond is None:
        body()
    else:
        pl.when(cond)(body)


def whole_kernel(Z, R, blocks, pairs, singles, refs):
    (
        q_in, k_in, v_in, g_in, u_in, d_in, resid_in, w_in, lam, head_gain, norm_gain,
        out,
        q_sc, kv_sc, wide_sc, thin_sc, resid, w,
        ho, heads, part, got, first, norm_sc, all_sc,
        hidden, acc, half, cross, rs_out, rs_in, res,
        zs, zr, ps, pr, pl_sem, local_sem, ho_sem, swap_sem, ag_sem, ag_land, core_sem,
        cross_sem, rs_sem, rs_land, out_sem,
    ) = refs
    z, r, t = where_am_i(R)
    me = z * R + r
    rx, ry = mirror_x(r), mirror_y(r)
    rd = mirror_x(ry)
    T = k_in.shape[0]
    D = resid_in.shape[1]
    DN = d_in.shape[1]
    H = T // 2
    ahead = [lax.rem(z + j, Z) for j in range(Z)]
    behind = [lax.rem(z + Z - j, Z) for j in range(Z)]
    chunks = pairs + singles
    uneven = blocks % Z != 0
    Q, KV = chunks, chunks + 1

    def dev(zz, rr):
        return zz * R + rr

    def span_of(c):
        return 2 if c < pairs else 1

    def offset(c):
        return 2 * c if c < pairs else pairs + c

    def store(o):
        if o == Q:
            return q_sc
        if o == KV:
            return kv_sc
        return wide_sc.at[o] if o < pairs else thin_sc.at[o - pairs]

    def present(o, zz):
        if not uneven or o != chunks - 1:
            return None
        count = block_start(blocks, Z, zz + 1) - block_start(blocks, Z, zz)
        return count > blocks // Z

    here = [present(o, z) for o in range(chunks + 2)]

    def parts(o, zz, slot):
        if o >= chunks:
            cols = pl.ds(pl.multiple_of(zz * VD, LANE), VD)
            if o == Q:
                return [(q_in.at[:, cols], q_sc.at[slot])]
            return [
                (ref.at[:, cols], kv_sc.at[slot, :, pl.ds(i * VD, VD)])
                for i, ref in enumerate((k_in, v_in))
            ]
        n = span_of(o)
        dst = store(o)
        start = pl.multiple_of((block_start(blocks, Z, zz) + offset(o)) * LANE, LANE)
        pairs_ = [
            (ref.at[:, pl.ds(start, n * LANE)], dst.at[slot, :, pl.ds(i * n * LANE, n * LANE)])
            for i, ref in enumerate((g_in, u_in))
        ]
        for i in range(n):
            rows = pl.ds(pl.multiple_of(start + i * LANE, LANE), LANE)
            pairs_.append((d_in.at[rows, :], dst.at[slot, :, pl.ds((2 * n + i) * LANE, LANE)]))
        return pairs_

    def slot_of(o, zz):
        return zz if o == Q else dev(zz, r)

    def zsend(o, j):
        return zs.at[o if here[o] is None else chunks + 1 + j]

    def first_hop(o, j):
        def body():
            for src, dst in parts(o, ahead[j], slot_of(o, z)):
                remote(src, dst, zsend(o, j), zr.at[o, j - 1], dev(ahead[j], r), t).start()

        when(present(o, ahead[j]), body)

    def arrived(o, j):
        spot = store(o).at[slot_of(o, behind[j])]

        def body():
            remote(spot, spot, zsend(o, j), zr.at[o, j - 1], dev(behind[j], r), t).wait_recv()

        when(here[o], body)

    def first_hops_sent(o):
        if here[o] is None:
            whole = store(o).at[pl.ds(0, Z - 1)]
            remote(whole, whole, zsend(o, 1), zr.at[o, 0], dev(ahead[1], r), t).wait_send()
            return
        for j in range(1, Z):
            spot = store(o).at[0]
            when(
                present(o, ahead[j]),
                lambda j=j: remote(
                    spot, spot, zsend(o, j), zr.at[o, j - 1], dev(ahead[j], r), t
                ).wait_send(),
            )

    def keep(o):
        def body():
            for src, dst in parts(o, z, slot_of(o, z)):
                pltpu.make_async_copy(src, dst, local_sem.at[o]).start()

        when(here[o], body)

    def kept(o):
        spot = store(o).at[slot_of(o, z)]
        when(here[o], lambda: pltpu.make_async_copy(spot, spot, local_sem.at[o]).wait())

    def piece(o, j, owner, h):
        ref = store(o)
        n = ref.shape[1] // 2
        return ref.at[dev(behind[j], owner), pl.ds(h * n, n), :]

    def psem(o):
        return o if o < chunks else chunks

    def landing(o, j, kind):
        p = psem(o)
        return pr.at[p, j] if kind in (0, 3) else pl_sem.at[p]

    def hop2(o, j, kind):
        owner = (r, r, r, r, rx, ry)[kind]
        target = (rx, rx, ry, ry, ry, rx)[kind]
        spot = piece(o, j, owner, kind % 2)
        return remote(spot, spot, ps.at[psem(o)], landing(o, j, kind), dev(z, target), t)

    def wait2(o, j):
        spot = store(o).at[dev(behind[j], rx)]
        remote(spot, spot, ps.at[psem(o)], landing(o, j, 0), dev(z, rx), t).wait_recv()

    def spread(o, j):
        if j:
            arrived(o, j)
        else:
            kept(o)

        def body():
            for kind in (0, 3, 1, 2):
                hop2(o, j, kind).start()

        when(here[o], body)

    def relay(o, j):
        def body():
            wait2(o, j)
            hop2(o, j, 4).start()
            hop2(o, j, 5).start()

        when(here[o], body)

    def settle(o):
        whole = store(o).at[pl.ds(0, 2 * Z)]
        when(
            here[o],
            lambda: remote(
                whole, whole, ps.at[psem(o)], landing(o, 0, 1), dev(z, rx), t
            ).wait_recv(),
        )

    def spread_sent(o):
        whole = store(o).at[pl.ds(0, 3 * Z)]
        when(
            here[o],
            lambda: remote(
                whole, whole, ps.at[psem(o)], landing(o, 0, 1), dev(z, rx), t
            ).wait_send(),
        )

    for o in (KV, *range(chunks), Q):
        keep(o)
    resid_copy = pltpu.make_async_copy(resid_in, resid, local_sem.at[chunks + 2])
    resid_copy.start()
    w_copy = pltpu.make_async_copy(w_in, w, local_sem.at[chunks + 3])
    w_copy.start()

    greet(
        [(dev(ahead[j], r), t) for j in range(1, Z)]
        + [(dev(z, rx), t), (dev(z, ry), t), (me, 1 - t)]
    )
    for o in (KV, 0, Q, 1):
        for j in range(1, Z):
            first_hop(o, j)
        if o == KV:
            spread(KV, 0)
    spread(0, 0)
    relay(KV, 0)
    for j in range(1, Z):
        spread(KV, j)
        if j > 1:
            relay(KV, j - 1)
        if j == Z - 2:
            spread(1, 0)
    relay(0, 0)
    relay(KV, Z - 1)
    for c in range(2, chunks):
        spread(c, 0)
    settle(KV)
    relay(1, 0)
    spread(0, 1)
    relay(2, 0)
    relay(3, 0)
    spread(0, 2)
    relay(0, 1)
    kept(Q)
    for j in range(1, Z):
        arrived(Q, j)

    head_lam = lam[z]

    def span(n, first_lane):
        return kv_sc[pl.ds(n * R, R), :, first_lane : first_lane + VD].reshape(R * T, VD)

    def ho_copy(i):
        return remote(ho.at[i], heads.at[z], ho_sem.at[Z], ho_sem.at[z], dev(i, r), t)

    for i in range(Z):
        ho[i] = attention_block(
            R, T, i, r,
            lambda b: q_sc[b],
            lambda n: span(n, 0),
            lambda n: span(n, VD),
            head_lam,
            head_gain[...],
        )

        @pl.when(z == i)
        def _(i=i):
            heads[i] = ho[i]

        pl.when(z != i)(lambda i=i: ho_copy(i).start())
        if i == 1:
            spread(0, 3)
        if i == 2:
            relay(0, 2)
    spread(1, 1)
    spread(1, 2)
    relay(0, 3)
    spread(1, 3)
    relay(1, 1)
    resid_copy.wait()
    w_copy.wait()
    for i in range(Z):

        @pl.when(z != i)
        def _(i=i):
            remote(
                ho.at[i], heads.at[i], ho_sem.at[Z], ho_sem.at[i], dev(i, r), t
            ).wait_recv()

    first_hop(2, 1)
    first_hop(2, 2)
    pl.when(z == 0)(lambda: first_hop(2, 3))
    NT = 512 if D % 512 == 0 else D
    for h in range(2):
        hh = (1 - t) if h == 0 else t
        rows = pl.ds(pl.multiple_of(hh * H, 16), H)
        left = jnp.concatenate([heads[n, rows, :] for n in range(Z)], axis=1)
        for n in range(0, D, NT):
            part[h, :, n : n + NT] = jnp.dot(
                left, w[:, n : n + NT], preferred_element_type=jnp.float32
            ).astype(jnp.bfloat16)
        if h == 0:
            swap = remote(part.at[0], got, swap_sem.at[0], swap_sem.at[1], me, 1 - t)
            swap.start()
    swap.wait()
    own_rows = pl.ds(pl.multiple_of(t * H, 16), H)
    first_val = resid[own_rows, :].astype(jnp.float32) + (
        part[1].astype(jnp.float32) + got[...].astype(jnp.float32)
    )
    first[...] = first_val
    norm_sc[...] = rms_rows(first_val, norm_gain[...])

    def rows_of(zz, tt):
        return all_sc.at[zz, tt]

    part_rows = H // SUB

    def ag_hop(down, d, s=None):
        zz = z + (d - 1) if down else z - (d - 1)
        to = z - 1 if down else z + 1
        src = norm_sc if d == 1 else rows_of(zz, t)
        dst = rows_of(zz, t)
        if s is not None:
            src, dst = (ref.at[pl.ds(s * part_rows, part_rows)] for ref in (src, dst))
        return remote(
            src, dst, ag_sem.at[down, d], ag_land.at[down, d, 0 if s is None else s], dev(to, r), t
        )

    def sends(down, d):
        return (z > 0) & (z + (d - 1) < Z) if down else (z + 1 < Z) & (z - (d - 1) >= 0)

    def gets(down, d):
        return z + d < Z if down else z - d >= 0

    def origin(down, d):
        return z + d if down else z - d

    def to_core(down, d, tt):
        rows = rows_of(origin(down, d), tt)
        n = 2 * d + down
        return remote(rows, rows, core_sem.at[2 * Z], core_sem.at[n], me, 1 - t)

    def ag_start(d):
        for s in range(SUB):
            for down in (0, 1):
                pl.when(sends(down, d))(lambda: ag_hop(down, d, s).start())

    def ag_step(d):
        for s in range(SUB):
            for down in (0, 1):

                @pl.when(gets(down, d))
                def _(down=down, s=s):
                    spot = rows_of(origin(down, d), t).at[pl.ds(s * part_rows, part_rows)]
                    remote(
                        spot, spot, ag_sem.at[down, d], ag_land.at[down, d, s], me, 1 - t
                    ).wait_recv()
                    if d < Z - 1:
                        pl.when(sends(down, d + 1))(lambda: ag_hop(down, d + 1, s).start())
                    if s == SUB - 1:
                        to_core(down, d, t).start()

    def ag_done(d):
        for down in (0, 1):

            @pl.when(gets(down, d))
            def _(down=down):
                to_core(down, d, 1 - t).wait_recv()

    def apply(cs, zz, fresh):
        block = all_sc[zz].reshape(T, D)
        lane = 0
        for c in cs:
            n = span_of(c) * LANE
            both = jnp.dot(
                block,
                store(c)[:, :, : 2 * n].reshape(D, 2 * n),
                preferred_element_type=jnp.float32,
            )
            value = jax.nn.silu(both[:, :n]) * both[:, n:]
            hidden[:, lane : lane + n] = value.astype(jnp.bfloat16)
            lane += n
        left = hidden[:, :lane]
        spots = [(c, 2 * span_of(c) + i) for c in cs for i in range(span_of(c))]
        group = 4 if (Z * R) % 8 == 0 else 1

        @pl.loop(0, (Z * R) // (2 * group))
        def _(g):
            for q in range(group):
                p = g * group + q
                right = jnp.concatenate(
                    [
                        jnp.concatenate(
                            [store(c)[2 * p + i, :, k * LANE : (k + 1) * LANE] for c, k in spots],
                            axis=0,
                        )
                        for i in range(2)
                    ],
                    axis=1,
                )
                value = jnp.dot(left, right, preferred_element_type=jnp.float32)
                cols = pl.ds(pl.multiple_of(p * (2 * DN), 2 * DN), 2 * DN)
                if fresh:
                    acc[zz, :, cols] = value
                else:
                    acc[zz, :, cols] = acc[zz, :, cols] + value

    early = tuple(range(pairs))
    late = tuple(range(pairs, chunks))

    def apply_near(cs, d, fresh):
        for down in (0, 1):

            @pl.when(gets(down, d))
            def _(down=down):
                apply(cs, origin(down, d), fresh)

    ag_start(1)
    across = remote(norm_sc, rows_of(z, t), core_sem.at[2 * Z], core_sem.at[0], me, 1 - t)
    across.start()
    own = pltpu.make_async_copy(norm_sc, rows_of(z, t), local_sem.at[0])
    own.start()
    pl.when(z > 0)(lambda: first_hop(2, 3))
    for j in range(1, Z):
        first_hop(3, j)
    relay(1, 2)
    spread(2, 1)
    spread(2, 2)
    relay(1, 3)
    settle(0)
    own.wait()
    remote(
        norm_sc, rows_of(z, 1 - t), core_sem.at[2 * Z], core_sem.at[0], me, 1 - t
    ).wait_recv()
    apply((0,), z, True)
    ag_step(1)
    spread(2, 3)
    relay(2, 1)
    ag_done(1)
    apply_near((0,), 1, True)
    spread(3, 1)
    spread(3, 2)
    relay(2, 2)
    spread(3, 3)
    relay(2, 3)
    settle(1)
    apply((1,), z, False)
    apply_near((1,), 1, False)
    ag_step(2)
    relay(3, 1)
    relay(3, 2)
    relay(3, 3)
    def pick(table):
        spot = jnp.int32(0)
        for zz in range(Z):
            spot = jnp.where(z == zz, table[zz], spot)
        return spot

    goals = [[1, Z - 1, *range(2, Z - 1)], [Z - 2, 0, *range(Z - 3, 0, -1)]]
    ranks = [[2, 3, 0, 1], [1, 0, 3, 2]]
    edge = (z == 0) | (z == Z - 1)
    fill = (3, 1)

    def cross_copy(zz):
        return remote(
            half.at[zz], cross.at[zz], cross_sem.at[Z], cross_sem.at[zz], me, 1 - t
        )

    other_rows = pl.ds(pl.multiple_of((1 - t) * H, 16), H)
    small = H // FINE

    def rs_copy(down, k, s):
        rows = pl.ds(s * small, small)
        to = z - 1 if down else z + 1
        return remote(
            rs_out.at[down, k, rows],
            rs_in.at[down, k, rows],
            rs_sem.at[down, k],
            rs_land.at[down, k, s],
            dev(to, r),
            t,
        )

    def rs_wait(down, k, s):
        rows = pl.ds(s * small, small)
        fro = z + 1 if down else z - 1
        remote(
            rs_out.at[down, k, rows],
            rs_in.at[down, k, rows],
            rs_sem.at[down, k],
            rs_land.at[down, k, s],
            dev(fro, r),
            t,
        ).wait_recv()

    def mine(zd, s):
        rows = pl.ds(s * small, small)
        long = pl.ds(pl.multiple_of(t * H + s * small, 16), small)
        return acc[zd, long, :] + cross[zd, rows, :].astype(jnp.float32)

    def hand_over(zz):
        half[zz] = acc[zz, other_rows, :].astype(jnp.bfloat16)
        cross_copy(zz).start()

    def rs_step(down, k, inner, subs=range(FINE)):
        zd = goals[down][k]
        for s in subs:
            rows = pl.ds(s * small, small)
            if s == 0:
                cross_copy(zd).wait_recv()
            total = mine(zd, s)
            if inner:
                rs_wait(down, k, s)
                total = total + rs_in[down, k, rows, :].astype(jnp.float32)
            rs_out[down, k, rows, :] = total.astype(jnp.bfloat16)
            rs_copy(down, k, s).start()

    def edge_step(k, low=(0, FINE), high=(0, FINE)):
        pl.when(z == 0)(lambda: rs_step(0, k, False, range(*low)))
        pl.when(z == Z - 1)(lambda: rs_step(1, k, False, range(*high)))

    @pl.when(edge)
    def _():
        settle(2)
        near = jnp.where(z == 0, 1, Z - 2)
        apply((2,), near, False)
        hand_over(near)

    ag_done(2)
    apply_near(early, 2, True)

    @pl.when(edge)
    def _():
        edge_step(0)
        mid = jnp.where(z == 0, 2, Z - 3)
        apply((2,), mid, False)
        hand_over(mid)
        apply((2,), z, False)
        hand_over(z)
        edge_step(2, (0, fill[0]), (0, fill[1]))
        for d in range(3, Z):
            ag_step(d)
            ag_done(d)
        far = jnp.where(z == 0, Z - 1, 0)
        apply(early + (2,), far, True)
        hand_over(far)
        edge_step(1)
        edge_step(2, (fill[0], FINE), (fill[1], FINE))

    @pl.when(jnp.logical_not(edge))
    def _():
        for c in late:
            settle(c)
        for n in range(Z):
            zz = jnp.where(z == 1, ranks[0][n], ranks[1][n])
            apply(late, zz, False)
            hand_over(zz)
        for low in (True, False):

            @pl.when(z == 1 if low else z == 2)
            def _(low=low):
                count = fill[0] if low else fill[1]
                first_way, second_way = (0, 1) if low else (1, 0)
                rs_step(first_way, 2, True, range(count))
                for s in range(FINE + 2):
                    if s < FINE:
                        rs_step(first_way, 1, True, (s,))
                    if s >= 2:
                        rs_step(second_way, 1, True, (s - 2,))
                rs_step(first_way, 2, True, range(count, FINE))


    cross_copy(z).wait_recv()
    for s in range(FINE):
        rows = pl.ds(s * small, small)
        first[rows, :] = first[rows, :] + 0.5 * mine(z, s)
        for down in (0, 1):

            @pl.when(z < Z - 1 if down else z > 0)
            def _(down=down, s=s, rows=rows):
                k = pick([goals[down].index(i) if i in goals[down] else 0 for i in range(Z)])
                rs_wait(down, k, s)
                first[rows, :] = first[rows, :] + 0.5 * rs_in[down, k, rows, :].astype(jnp.float32)

        res[rows, :] = first[rows, :].astype(jnp.bfloat16)
        place = out.at[pl.ds(pl.multiple_of(t * H + s * small, 16), small), :]
        remote(res.at[rows], place, out_sem.at[0], out_sem.at[1], me, 1 - t).start()
        pltpu.make_async_copy(res.at[rows], place, local_sem.at[1]).start()
    theirs = out.at[pl.ds(pl.multiple_of((1 - t) * H, 16), H), :]
    remote(res, theirs, out_sem.at[0], out_sem.at[1], me, 1 - t).wait()
    pltpu.make_async_copy(res, out.at[own_rows, :], local_sem.at[1]).wait()
    remote(half, cross, cross_sem.at[Z], cross_sem.at[0], me, 1 - t).wait_send()
    remote(half, cross, core_sem.at[2 * Z], core_sem.at[0], me, 1 - t).wait_send()
    for d in range(1, Z):
        for down in (0, 1):

            @pl.when(sends(down, d))
            def _(down=down, d=d):
                ag_hop(down, d).wait_send()

    for k in range(Z - 1):
        for down in (0, 1):
            zd = goals[down][k]

            @pl.when(z > zd if down else z < zd)
            def _(down=down, k=k):
                whole = rs_out.at[down, k]
                remote(whole, whole, rs_sem.at[down, k], rs_land.at[down, k, 0], me, 1 - t).wait_send()

    for o in (KV, Q, *range(chunks)):
        first_hops_sent(o)
    for o in (KV, *range(chunks)):
        spread_sent(o)
    sent = ho.at[pl.ds(0, Z - 1)]
    remote(sent, sent, ho_sem.at[Z], ho_sem.at[0], me, 1 - t).wait_send()


def columns_form(
    resid,
    queries,
    keys,
    values,
    lambdas,
    head_gain,
    out_weight,
    norm_gain,
    gate_weight,
    up_weight,
    down_weight,
):
    Z = lambdas.shape[0]
    S = lax.axis_size("sp")
    R = S // Z
    T, D = resid.shape
    H = T // 2
    W = gate_weight.shape[0]
    DN = down_weight.shape[1]
    blocks = gate_weight.shape[1] // LANE
    pairs = blocks // Z // 2
    singles = blocks // Z % 2 + (1 if blocks % Z else 0)
    chunks = pairs + singles
    bf, f32 = jnp.bfloat16, jnp.float32
    vm = pl.BlockSpec(memory_space=pltpu.VMEM)
    hbm = pl.BlockSpec(memory_space=pl.ANY)
    dma = pltpu.SemaphoreType.DMA

    def kernel(*refs):
        whole_kernel(Z, R, blocks, pairs, singles, refs)

    return pl.pallas_call(
        kernel,
        out_shape=pltpu.VMEM((T, D), bf),
        in_specs=[hbm] * 8 + [pl.BlockSpec(memory_space=pltpu.SMEM), vm, vm],
        out_specs=vm,
        scratch_shapes=[
            pltpu.VMEM((Z, T, VD), bf),
            pltpu.VMEM((S, T, 2 * VD), bf),
            pltpu.VMEM((pairs, S, W, 6 * LANE), bf),
            pltpu.VMEM((singles, S, W, 3 * LANE), bf),
            pltpu.VMEM((T, D), bf),
            pltpu.VMEM(out_weight.shape, bf),
            pltpu.VMEM((Z, T, VD), bf),
            pltpu.VMEM((Z, T, VD), bf),
            pltpu.VMEM((2, H, D), bf),
            pltpu.VMEM((H, D), bf),
            pltpu.VMEM((H, D), f32),
            pltpu.VMEM((H, D), bf),
            pltpu.VMEM((Z, 2, H, D), bf),
            pltpu.VMEM((T, (2 * pairs + singles) * LANE), bf),
            pltpu.VMEM((Z, T, D), f32),
            pltpu.VMEM((Z, H, D), bf),
            pltpu.VMEM((Z, H, D), bf),
            pltpu.VMEM((2, Z - 1, H, D), bf),
            pltpu.VMEM((2, Z - 1, H, D), bf),
            pltpu.VMEM((H, D), bf),
            dma((chunks + 1 + Z,)),
            dma((chunks + 2, Z - 1)),
            dma((chunks + 1,)),
            dma((chunks + 1, Z)),
            dma((chunks + 1,)),
            dma((chunks + 4,)),
            dma((Z + 1,)),
            dma((2,)),
            dma((2, Z)),
            dma((2, Z, SUB)),
            dma((2 * Z + 1,)),
            dma((Z + 1,)),
            dma((2, Z - 1)),
            dma((2, Z - 1, FINE)),
            dma((2,)),
        ],
        compiler_params=pltpu.CompilerParams(
            collective_id=0, has_side_effects=True, vmem_limit_bytes=VMEM_LIMIT
        ),
    )(
        queries,
        keys,
        values,
        gate_weight,
        up_weight,
        down_weight,
        resid,
        out_weight,
        lambdas,
        head_gain.reshape(1, -1),
        norm_gain.reshape(1, -1),
    )


def solution(mesh):
    sp, tp = mesh.shape["sp"], mesh.shape["tp"]

    def local(*args):
        heads = args[4].shape[0]
        tok_rows = args[1].shape[0]
        columns = (
            tp == 2
            and heads == 4
            and sp == 4 * heads
            and args[10].shape[1] == LANE
            and args[8].shape[0] == LANE
            and args[8].shape[1] % LANE == 0
            and args[8].shape[1] // LANE // heads == 5
            and args[8].shape[1] // LANE % heads == 2
            and tok_rows % (32 * FINE) == 0
            and FINE % SUB == 0
        )
        return (columns_form if columns else generic)(*args)

    return jax.shard_map(
        local,
        mesh=mesh,
        in_specs=(
            P("sp", None),
            P("sp", "tp"),
            P("sp", "tp"),
            P("sp", "tp"),
            P("tp"),
            P(),
            P("tp", None),
            P(),
            P("sp", "tp"),
            P("sp", "tp"),
            P("tp", "sp"),
        ),
        out_specs=P("sp", None),
        check_vma=False,
    )
```

```python
import jax
import jax.numpy as jnp
from jax import lax
from jax.experimental import pallas as pl
from jax.experimental.pallas import tpu as pltpu
from jax.sharding import PartitionSpec as P

QK = 64
VD = 128
LANE = 128
SUB = 3
FINE = 6
VMEM_LIMIT = 60 * 1024 * 1024


def rms_rows(first, norm_gain):
    return (
        first * lax.rsqrt(jnp.mean(first * first, axis=-1, keepdims=True) + 1e-06) * norm_gain
    ).astype(jnp.bfloat16)


def generic(
    resid,
    queries,
    keys,
    values,
    lambdas,
    head_gain,
    out_weight,
    norm_gain,
    gate_weight,
    up_weight,
    down_weight,
):
    tok_rows = queries.shape[0]
    local_heads = lambdas.shape[0]
    model_width = resid.shape[1]
    offset = lax.axis_index("sp") * tok_rows
    query_four = queries.reshape(tok_rows, local_heads, 2, QK)
    score_scale = QK ** (-0.5)
    query_pos = offset + lax.iota(jnp.int32, tok_rows)

    def update(fold_state, key_part, value_part, key_pos):
        run_max, run_sum, run_acc = fold_state
        scores = (
            jnp.einsum("qhcd,khcd->chqk", query_four, key_part, preferred_element_type=jnp.float32)
            * score_scale
        )
        causal_mask = key_pos[None, :] <= query_pos[:, None]
        scores = jnp.where(causal_mask, scores, -1e30)
        new_max = jnp.maximum(run_max, jnp.max(scores, axis=-1))
        expo = jnp.where(causal_mask, jnp.exp(scores - new_max[..., None]), 0.0)
        factor = jnp.exp(run_max - new_max)
        new_sum = run_sum * factor + jnp.sum(expo, axis=-1)
        new_acc = run_acc * factor[..., None] + jnp.einsum(
            "chqk,khd->chqd",
            expo.astype(jnp.bfloat16),
            value_part,
            preferred_element_type=jnp.float32,
        )
        return (new_max, new_sum, new_acc)

    initial = (
        jnp.full((2, local_heads, tok_rows), -1e30, jnp.float32),
        jnp.zeros((2, local_heads, tok_rows), jnp.float32),
        jnp.zeros((2, local_heads, tok_rows, VD), jnp.float32),
    )
    key_rows = lax.all_gather(keys, "sp", axis=0, tiled=True)
    value_rows = lax.all_gather(values, "sp", axis=0, tiled=True)
    key_count = key_rows.shape[0]
    key_span = key_count
    while key_span > 1024 and key_span % 2 == 0:
        key_span = key_span // 2

    def one_span(span_index, inner_state):
        span_start = span_index * key_span
        key_part = lax.dynamic_slice_in_dim(key_rows, span_start, key_span, 0).reshape(
            key_span, local_heads, 2, QK
        )
        value_part = lax.dynamic_slice_in_dim(value_rows, span_start, key_span, 0).reshape(
            key_span, local_heads, VD
        )
        key_pos = span_start + lax.iota(jnp.int32, key_span)
        return update(inner_state, key_part, value_part, key_pos)

    final_max, final_sum, final_acc = lax.fori_loop(0, key_count // key_span, one_span, initial)
    ratio = final_acc / final_sum[..., None]
    mixed_heads = ratio[0] - lambdas[:, None, None] * ratio[1]
    head_out = (
        mixed_heads
        * lax.rsqrt(jnp.mean(mixed_heads * mixed_heads, axis=-1, keepdims=True) + 1e-05)
        * head_gain
    ).astype(jnp.bfloat16)
    out_three = out_weight.reshape(local_heads, VD, model_width)
    own_count = tok_rows // lax.axis_size("tp")
    branch = lax.psum_scatter(
        jnp.einsum("hqd,hde->qe", head_out, out_three, preferred_element_type=jnp.float32).astype(
            jnp.bfloat16
        ),
        "tp",
        scatter_dimension=0,
        tiled=True,
    ).astype(jnp.float32)
    resid_own = lax.dynamic_slice_in_dim(resid, lax.axis_index("tp") * own_count, own_count, 0)
    first = resid_own.astype(jnp.float32) + branch
    normed_all = lax.all_gather(rms_rows(first, norm_gain), "tp", axis=0, tiled=True)
    gate_act = jnp.dot(
        normed_all,
        lax.all_gather(gate_weight, "sp", axis=0, tiled=True),
        preferred_element_type=jnp.float32,
    )
    up_act = jnp.dot(
        normed_all,
        lax.all_gather(up_weight, "sp", axis=0, tiled=True),
        preferred_element_type=jnp.float32,
    )
    hidden = (jax.nn.silu(gate_act) * up_act).astype(jnp.bfloat16)
    terms = jnp.dot(
        hidden,
        lax.all_gather(down_weight, "sp", axis=1, tiled=True),
        preferred_element_type=jnp.float32,
    )
    mixer = lax.psum_scatter(
        terms.astype(jnp.bfloat16), "tp", scatter_dimension=0, tiled=True
    ).astype(jnp.float32)
    finished = (first + 0.5 * mixer).astype(jnp.bfloat16)
    return lax.all_gather(finished, "tp", axis=0, tiled=True)


def where_am_i(R):
    s = lax.axis_index("sp")
    return s // R, lax.rem(s, R), lax.axis_index("tp")


def remote(src, dst, send, recv, sp, tp):
    return pltpu.make_async_remote_copy(
        src_ref=src,
        dst_ref=dst,
        send_sem=send,
        recv_sem=recv,
        device_id={"sp": sp, "tp": tp},
        device_id_type=pl.DeviceIdType.MESH,
    )


def greet(peers):
    barrier = pltpu.get_barrier_semaphore()
    for sp, tp in peers:
        pl.semaphore_signal(
            barrier,
            inc=1,
            device_id={"sp": sp, "tp": tp},
            device_id_type=pl.DeviceIdType.MESH,
        )
    pl.semaphore_wait(barrier, len(peers))


def mirror_x(r):
    return r + 1 - 2 * lax.rem(r, 2)


def mirror_y(r):
    return r + 2 - 4 * (lax.rem(r, 4) // 2)


def attention_block(R, T, i, r, q_at, k_at, v_at, lam, gain):
    span = R * T
    query = q_at(i) * jnp.bfloat16(QK**-0.5)
    ratios = []
    for c in range(2):
        part = query[:, c * QK : (c + 1) * QK]

        def fold(n, state, masked):
            run_max, run_sum, run_acc = state
            key = k_at(n)[:, c * QK : (c + 1) * QK]
            scores = lax.dot_general(
                part, key, (((1,), (1,)), ((), ())), preferred_element_type=jnp.float32
            )
            if masked:
                qpos = r * T + lax.broadcasted_iota(jnp.int32, scores.shape, 0)
                kpos = lax.broadcasted_iota(jnp.int32, scores.shape, 1)
                scores = jnp.where(kpos <= qpos, scores, -1e30)
            new_max = jnp.maximum(run_max, jnp.max(scores, axis=-1, keepdims=True))
            expo = jnp.exp(scores - new_max)
            factor = jnp.exp(run_max - new_max)
            new_sum = run_sum * factor + jnp.sum(expo, axis=-1, keepdims=True)
            new_acc = run_acc * factor + jnp.dot(
                expo.astype(jnp.bfloat16), v_at(n), preferred_element_type=jnp.float32
            )
            return new_max, new_sum, new_acc

        state = (
            jnp.full((T, 1), -1e30, jnp.float32),
            jnp.zeros((T, 1), jnp.float32),
            jnp.zeros((T, VD), jnp.float32),
        )
        state = fold(i, state, True)
        state = lax.fori_loop(0, i, lambda n, st: fold(n, st, False), state)
        ratios.append(state[2] / state[1])
    mixed = ratios[0] - lam * ratios[1]
    return (
        mixed * lax.rsqrt(jnp.mean(mixed * mixed, axis=-1, keepdims=True) + 1e-05) * gain
    ).astype(jnp.bfloat16)


def block_start(blocks, Z, zz):
    extra = blocks % Z
    return blocks // Z * zz + jnp.minimum(jnp.maximum(zz - (Z - extra) // 2, 0), extra)


def when(cond, body):
    if cond is None:
        body()
    else:
        pl.when(cond)(body)


def whole_kernel(Z, R, blocks, pairs, singles, refs):
    (
        q_in, k_in, v_in, g_in, u_in, d_in, resid_in, w_in, lam, head_gain, norm_gain,
        out,
        q_sc, kv_sc, wide_sc, thin_sc, resid, w,
        ho, heads, part, got, first, norm_sc, all_sc,
        hidden, acc, half, cross, rs_out, rs_in, res,
        zs, zr, ps, pr, pl_sem, local_sem, ho_sem, swap_sem, ag_sem, ag_land, core_sem,
        cross_sem, rs_sem, rs_land, out_sem,
    ) = refs
    z, r, t = where_am_i(R)
    me = z * R + r
    rx, ry = mirror_x(r), mirror_y(r)
    rd = mirror_x(ry)
    T = k_in.shape[0]
    D = resid_in.shape[1]
    DN = d_in.shape[1]
    H = T // 2
    ahead = [lax.rem(z + j, Z) for j in range(Z)]
    behind = [lax.rem(z + Z - j, Z) for j in range(Z)]
    chunks = pairs + singles
    uneven = blocks % Z != 0
    Q, KV = chunks, chunks + 1

    def dev(zz, rr):
        return zz * R + rr

    def span_of(c):
        return 2 if c < pairs else 1

    def offset(c):
        return 2 * c if c < pairs else pairs + c

    def store(o):
        if o == Q:
            return q_sc
        if o == KV:
            return kv_sc
        return wide_sc.at[o] if o < pairs else thin_sc.at[o - pairs]

    def present(o, zz):
        if not uneven or o != chunks - 1:
            return None
        count = block_start(blocks, Z, zz + 1) - block_start(blocks, Z, zz)
        return count > blocks // Z

    here = [present(o, z) for o in range(chunks + 2)]

    def parts(o, zz, slot):
        if o >= chunks:
            cols = pl.ds(pl.multiple_of(zz * VD, LANE), VD)
            if o == Q:
                return [(q_in.at[:, cols], q_sc.at[slot])]
            return [
                (ref.at[:, cols], kv_sc.at[slot, :, pl.ds(i * VD, VD)])
                for i, ref in enumerate((k_in, v_in))
            ]
        n = span_of(o)
        dst = store(o)
        start = pl.multiple_of((block_start(blocks, Z, zz) + offset(o)) * LANE, LANE)
        pairs_ = [
            (ref.at[:, pl.ds(start, n * LANE)], dst.at[slot, :, pl.ds(i * n * LANE, n * LANE)])
            for i, ref in enumerate((g_in, u_in))
        ]
        for i in range(n):
            rows = pl.ds(pl.multiple_of(start + i * LANE, LANE), LANE)
            pairs_.append((d_in.at[rows, :], dst.at[slot, :, pl.ds((2 * n + i) * LANE, LANE)]))
        return pairs_

    def slot_of(o, zz):
        return zz if o == Q else dev(zz, r)

    def zsend(o, j):
        return zs.at[o if here[o] is None else chunks + 1 + j]

    def first_hop(o, j):
        def body():
            for src, dst in parts(o, ahead[j], slot_of(o, z)):
                remote(src, dst, zsend(o, j), zr.at[o, j - 1], dev(ahead[j], r), t).start()

        when(present(o, ahead[j]), body)

    def arrived(o, j):
        spot = store(o).at[slot_of(o, behind[j])]

        def body():
            remote(spot, spot, zsend(o, j), zr.at[o, j - 1], dev(behind[j], r), t).wait_recv()

        when(here[o], body)

    def first_hops_sent(o):
        if here[o] is None:
            whole = store(o).at[pl.ds(0, Z - 1)]
            remote(whole, whole, zsend(o, 1), zr.at[o, 0], dev(ahead[1], r), t).wait_send()
            return
        for j in range(1, Z):
            spot = store(o).at[0]
            when(
                present(o, ahead[j]),
                lambda j=j: remote(
                    spot, spot, zsend(o, j), zr.at[o, j - 1], dev(ahead[j], r), t
                ).wait_send(),
            )

    def keep(o):
        def body():
            for src, dst in parts(o, z, slot_of(o, z)):
                pltpu.make_async_copy(src, dst, local_sem.at[o]).start()

        when(here[o], body)

    def kept(o):
        spot = store(o).at[slot_of(o, z)]
        when(here[o], lambda: pltpu.make_async_copy(spot, spot, local_sem.at[o]).wait())

    def piece(o, j, owner, h):
        ref = store(o)
        n = ref.shape[1] // 2
        return ref.at[dev(behind[j], owner), pl.ds(h * n, n), :]

    def psem(o):
        return o if o < chunks else chunks

    def landing(o, j, kind):
        p = psem(o)
        return pr.at[p, j] if kind in (0, 3) else pl_sem.at[p]

    def hop2(o, j, kind):
        owner = (r, r, r, r, rx, ry)[kind]
        target = (rx, rx, ry, ry, ry, rx)[kind]
        spot = piece(o, j, owner, kind % 2)
        return remote(spot, spot, ps.at[psem(o)], landing(o, j, kind), dev(z, target), t)

    def wait2(o, j):
        spot = store(o).at[dev(behind[j], rx)]
        remote(spot, spot, ps.at[psem(o)], landing(o, j, 0), dev(z, rx), t).wait_recv()

    def spread(o, j):
        if j:
            arrived(o, j)
        else:
            kept(o)

        def body():
            for kind in (0, 3, 1, 2):
                hop2(o, j, kind).start()

        when(here[o], body)

    def relay(o, j):
        def body():
            wait2(o, j)
            hop2(o, j, 4).start()
            hop2(o, j, 5).start()

        when(here[o], body)

    def settle(o):
        whole = store(o).at[pl.ds(0, 2 * Z)]
        when(
            here[o],
            lambda: remote(
                whole, whole, ps.at[psem(o)], landing(o, 0, 1), dev(z, rx), t
            ).wait_recv(),
        )

    def spread_sent(o):
        whole = store(o).at[pl.ds(0, 3 * Z)]
        when(
            here[o],
            lambda: remote(
                whole, whole, ps.at[psem(o)], landing(o, 0, 1), dev(z, rx), t
            ).wait_send(),
        )

    for o in (KV, *range(chunks), Q):
        keep(o)
    resid_copy = pltpu.make_async_copy(resid_in, resid, local_sem.at[chunks + 2])
    resid_copy.start()
    w_copy = pltpu.make_async_copy(w_in, w, local_sem.at[chunks + 3])
    w_copy.start()

    greet(
        [(dev(ahead[j], r), t) for j in range(1, Z)]
        + [(dev(z, rx), t), (dev(z, ry), t), (me, 1 - t)]
    )
    for o in (KV, 0, Q, 1):
        for j in range(1, Z):
            first_hop(o, j)
        if o == KV:
            spread(KV, 0)
    spread(0, 0)
    relay(KV, 0)
    for j in range(1, Z):
        spread(KV, j)
        if j > 1:
            relay(KV, j - 1)
        if j == Z - 2:
            spread(1, 0)
    relay(0, 0)
    relay(KV, Z - 1)
    for c in range(2, chunks):
        spread(c, 0)
    settle(KV)
    relay(1, 0)
    spread(0, 1)
    relay(2, 0)
    relay(3, 0)
    spread(0, 2)
    relay(0, 1)
    kept(Q)
    for j in range(1, Z):
        arrived(Q, j)

    head_lam = lam[z]

    def span(n, first_lane):
        return kv_sc[pl.ds(n * R, R), :, first_lane : first_lane + VD].reshape(R * T, VD)

    def ho_copy(i):
        return remote(ho.at[i], heads.at[z], ho_sem.at[Z], ho_sem.at[z], dev(i, r), t)

    for i in range(Z):
        ho[i] = attention_block(
            R, T, i, r,
            lambda b: q_sc[b],
            lambda n: span(n, 0),
            lambda n: span(n, VD),
            head_lam,
            head_gain[...],
        )

        @pl.when(z == i)
        def _(i=i):
            heads[i] = ho[i]

        pl.when(z != i)(lambda i=i: ho_copy(i).start())
        if i == 1:
            spread(0, 3)
        if i == 2:
            relay(0, 2)
    first_hop(2, 1)
    first_hop(2, 2)
    spread(1, 1)
    spread(1, 2)
    relay(0, 3)
    resid_copy.wait()
    w_copy.wait()
    for i in range(Z):

        @pl.when(z != i)
        def _(i=i):
            remote(
                ho.at[i], heads.at[i], ho_sem.at[Z], ho_sem.at[i], dev(i, r), t
            ).wait_recv()

    pl.when(z == 0)(lambda: first_hop(2, 3))
    NT = 512 if D % 512 == 0 else D
    for h in range(2):
        hh = (1 - t) if h == 0 else t
        rows = pl.ds(pl.multiple_of(hh * H, 16), H)
        left = jnp.concatenate([heads[n, rows, :] for n in range(Z)], axis=1)
        for n in range(0, D, NT):
            part[h, :, n : n + NT] = jnp.dot(
                left, w[:, n : n + NT], preferred_element_type=jnp.float32
            ).astype(jnp.bfloat16)
        if h == 0:
            swap = remote(part.at[0], got, swap_sem.at[0], swap_sem.at[1], me, 1 - t)
            swap.start()
    swap.wait()
    own_rows = pl.ds(pl.multiple_of(t * H, 16), H)
    first_val = resid[own_rows, :].astype(jnp.float32) + (
        part[1].astype(jnp.float32) + got[...].astype(jnp.float32)
    )
    first[...] = first_val
    norm_sc[...] = rms_rows(first_val, norm_gain[...])

    def rows_of(zz, tt):
        return all_sc.at[zz, tt]

    part_rows = H // SUB

    def ag_hop(down, d, s=None):
        zz = z + (d - 1) if down else z - (d - 1)
        to = z - 1 if down else z + 1
        src = norm_sc if d == 1 else rows_of(zz, t)
        dst = rows_of(zz, t)
        if s is not None:
            src, dst = (ref.at[pl.ds(s * part_rows, part_rows)] for ref in (src, dst))
        return remote(
            src, dst, ag_sem.at[down, d], ag_land.at[down, d, 0 if s is None else s], dev(to, r), t
        )

    def sends(down, d):
        return (z > 0) & (z + (d - 1) < Z) if down else (z + 1 < Z) & (z - (d - 1) >= 0)

    def gets(down, d):
        return z + d < Z if down else z - d >= 0

    def origin(down, d):
        return z + d if down else z - d

    def to_core(down, d, tt):
        rows = rows_of(origin(down, d), tt)
        n = 2 * d + down
        return remote(rows, rows, core_sem.at[2 * Z], core_sem.at[n], me, 1 - t)

    def ag_start(d):
        for s in range(SUB):
            for down in (0, 1):
                pl.when(sends(down, d))(lambda: ag_hop(down, d, s).start())

    def ag_step(d):
        for s in range(SUB):
            for down in (0, 1):

                @pl.when(gets(down, d))
                def _(down=down, s=s):
                    spot = rows_of(origin(down, d), t).at[pl.ds(s * part_rows, part_rows)]
                    remote(
                        spot, spot, ag_sem.at[down, d], ag_land.at[down, d, s], me, 1 - t
                    ).wait_recv()
                    if d < Z - 1:
                        pl.when(sends(down, d + 1))(lambda: ag_hop(down, d + 1, s).start())
                    if s == SUB - 1:
                        to_core(down, d, t).start()

    def ag_done(d):
        for down in (0, 1):

            @pl.when(gets(down, d))
            def _(down=down):
                to_core(down, d, 1 - t).wait_recv()

    def apply(cs, zz, fresh):
        block = all_sc[zz].reshape(T, D)
        lane = 0
        for c in cs:
            n = span_of(c) * LANE
            both = jnp.dot(
                block,
                store(c)[:, :, : 2 * n].reshape(D, 2 * n),
                preferred_element_type=jnp.float32,
            )
            value = jax.nn.silu(both[:, :n]) * both[:, n:]
            hidden[:, lane : lane + n] = value.astype(jnp.bfloat16)
            lane += n
        left = hidden[:, :lane]
        spots = [(c, 2 * span_of(c) + i) for c in cs for i in range(span_of(c))]
        group = 4 if (Z * R) % 8 == 0 else 1

        @pl.loop(0, (Z * R) // (2 * group))
        def _(g):
            for q in range(group):
                p = g * group + q
                right = jnp.concatenate(
                    [
                        jnp.concatenate(
                            [store(c)[2 * p + i, :, k * LANE : (k + 1) * LANE] for c, k in spots],
                            axis=0,
                        )
                        for i in range(2)
                    ],
                    axis=1,
                )
                value = jnp.dot(left, right, preferred_element_type=jnp.float32)
                cols = pl.ds(pl.multiple_of(p * (2 * DN), 2 * DN), 2 * DN)
                if fresh:
                    acc[zz, :, cols] = value
                else:
                    acc[zz, :, cols] = acc[zz, :, cols] + value

    early = tuple(range(pairs))
    late = tuple(range(pairs, chunks))

    def apply_near(cs, d, fresh):
        for down in (0, 1):

            @pl.when(gets(down, d))
            def _(down=down):
                apply(cs, origin(down, d), fresh)

    ag_start(1)
    across = remote(norm_sc, rows_of(z, t), core_sem.at[2 * Z], core_sem.at[0], me, 1 - t)
    across.start()
    own = pltpu.make_async_copy(norm_sc, rows_of(z, t), local_sem.at[0])
    own.start()
    pl.when(z > 0)(lambda: first_hop(2, 3))
    for j in range(1, Z):
        first_hop(3, j)
    spread(1, 3)
    relay(1, 1)
    relay(1, 2)
    spread(2, 1)
    spread(2, 2)
    relay(1, 3)
    settle(0)
    own.wait()
    remote(
        norm_sc, rows_of(z, 1 - t), core_sem.at[2 * Z], core_sem.at[0], me, 1 - t
    ).wait_recv()
    apply((0,), z, True)
    ag_step(1)
    spread(2, 3)
    relay(2, 1)
    ag_done(1)
    apply_near((0,), 1, True)
    spread(3, 1)
    spread(3, 2)
    relay(2, 2)
    spread(3, 3)
    relay(2, 3)
    settle(1)
    apply((1,), z, False)
    apply_near((1,), 1, False)
    ag_step(2)
    relay(3, 1)
    relay(3, 2)
    relay(3, 3)
    def pick(table):
        spot = jnp.int32(0)
        for zz in range(Z):
            spot = jnp.where(z == zz, table[zz], spot)
        return spot

    goals = [[1, Z - 1, *range(2, Z - 1)], [Z - 2, 0, *range(Z - 3, 0, -1)]]
    ranks = [[2, 3, 0, 1], [1, 0, 3, 2]]
    edge = (z == 0) | (z == Z - 1)
    fill = (3, 2)

    def cross_copy(zz):
        return remote(
            half.at[zz], cross.at[zz], cross_sem.at[Z], cross_sem.at[zz], me, 1 - t
        )

    other_rows = pl.ds(pl.multiple_of((1 - t) * H, 16), H)
    small = H // FINE

    def rs_copy(down, k, s):
        rows = pl.ds(s * small, small)
        to = z - 1 if down else z + 1
        return remote(
            rs_out.at[down, k, rows],
            rs_in.at[down, k, rows],
            rs_sem.at[down, k],
            rs_land.at[down, k, s],
            dev(to, r),
            t,
        )

    def rs_wait(down, k, s):
        rows = pl.ds(s * small, small)
        fro = z + 1 if down else z - 1
        remote(
            rs_out.at[down, k, rows],
            rs_in.at[down, k, rows],
            rs_sem.at[down, k],
            rs_land.at[down, k, s],
            dev(fro, r),
            t,
        ).wait_recv()

    def mine(zd, s):
        rows = pl.ds(s * small, small)
        long = pl.ds(pl.multiple_of(t * H + s * small, 16), small)
        return acc[zd, long, :] + cross[zd, rows, :].astype(jnp.float32)

    def hand_over(zz):
        half[zz] = acc[zz, other_rows, :].astype(jnp.bfloat16)
        cross_copy(zz).start()

    def rs_step(down, k, inner, subs=range(FINE)):
        zd = goals[down][k]
        for s in subs:
            rows = pl.ds(s * small, small)
            if s == 0:
                cross_copy(zd).wait_recv()
            total = mine(zd, s)
            if inner:
                rs_wait(down, k, s)
                total = total + rs_in[down, k, rows, :].astype(jnp.float32)
            rs_out[down, k, rows, :] = total.astype(jnp.bfloat16)
            rs_copy(down, k, s).start()

    def edge_step(k, low=(0, FINE), high=(0, FINE)):
        pl.when(z == 0)(lambda: rs_step(0, k, False, range(*low)))
        pl.when(z == Z - 1)(lambda: rs_step(1, k, False, range(*high)))

    @pl.when(edge)
    def _():
        settle(2)
        near = jnp.where(z == 0, 1, Z - 2)
        apply((2,), near, False)
        hand_over(near)

    ag_done(2)
    apply_near(early, 2, True)

    @pl.when(edge)
    def _():
        edge_step(0)
        mid = jnp.where(z == 0, 2, Z - 3)
        apply((2,), mid, False)
        hand_over(mid)
        apply((2,), z, False)
        hand_over(z)
        edge_step(2, (0, fill[0]), (0, fill[1]))
        for d in range(3, Z):
            ag_step(d)
            ag_done(d)
        far = jnp.where(z == 0, Z - 1, 0)
        apply(early + (2,), far, True)
        hand_over(far)
        edge_step(1)
        edge_step(2, (fill[0], FINE), (fill[1], FINE))

    @pl.when(jnp.logical_not(edge))
    def _():
        for c in late:
            settle(c)
        for n in range(Z):
            zz = jnp.where(z == 1, ranks[0][n], ranks[1][n])
            apply(late, zz, False)
            hand_over(zz)
        for low in (True, False):

            @pl.when(z == 1 if low else z == 2)
            def _(low=low):
                count = fill[0] if low else fill[1]
                first_way, second_way = (0, 1) if low else (1, 0)
                rs_step(first_way, 2, True, range(count))
                for s in range(FINE + 2):
                    if s < FINE:
                        rs_step(first_way, 1, True, (s,))
                    if s >= 2:
                        rs_step(second_way, 1, True, (s - 2,))
                rs_step(first_way, 2, True, range(count, FINE))


    cross_copy(z).wait_recv()
    for s in range(FINE):
        rows = pl.ds(s * small, small)
        first[rows, :] = first[rows, :] + 0.5 * mine(z, s)
        for down in (0, 1):

            @pl.when(z < Z - 1 if down else z > 0)
            def _(down=down, s=s, rows=rows):
                k = pick([goals[down].index(i) if i in goals[down] else 0 for i in range(Z)])
                rs_wait(down, k, s)
                first[rows, :] = first[rows, :] + 0.5 * rs_in[down, k, rows, :].astype(jnp.float32)

        res[rows, :] = first[rows, :].astype(jnp.bfloat16)
        place = out.at[pl.ds(pl.multiple_of(t * H + s * small, 16), small), :]
        remote(res.at[rows], place, out_sem.at[0], out_sem.at[1], me, 1 - t).start()
        pltpu.make_async_copy(res.at[rows], place, local_sem.at[1]).start()
    theirs = out.at[pl.ds(pl.multiple_of((1 - t) * H, 16), H), :]
    remote(res, theirs, out_sem.at[0], out_sem.at[1], me, 1 - t).wait()
    pltpu.make_async_copy(res, out.at[own_rows, :], local_sem.at[1]).wait()
    remote(half, cross, cross_sem.at[Z], cross_sem.at[0], me, 1 - t).wait_send()
    remote(half, cross, core_sem.at[2 * Z], core_sem.at[0], me, 1 - t).wait_send()
    for d in range(1, Z):
        for down in (0, 1):

            @pl.when(sends(down, d))
            def _(down=down, d=d):
                ag_hop(down, d).wait_send()

    for k in range(Z - 1):
        for down in (0, 1):
            zd = goals[down][k]

            @pl.when(z > zd if down else z < zd)
            def _(down=down, k=k):
                whole = rs_out.at[down, k]
                remote(whole, whole, rs_sem.at[down, k], rs_land.at[down, k, 0], me, 1 - t).wait_send()

    for o in (KV, Q, *range(chunks)):
        first_hops_sent(o)
    for o in (KV, *range(chunks)):
        spread_sent(o)
    sent = ho.at[pl.ds(0, Z - 1)]
    remote(sent, sent, ho_sem.at[Z], ho_sem.at[0], me, 1 - t).wait_send()


def columns_form(
    resid,
    queries,
    keys,
    values,
    lambdas,
    head_gain,
    out_weight,
    norm_gain,
    gate_weight,
    up_weight,
    down_weight,
):
    Z = lambdas.shape[0]
    S = lax.axis_size("sp")
    R = S // Z
    T, D = resid.shape
    H = T // 2
    W = gate_weight.shape[0]
    DN = down_weight.shape[1]
    blocks = gate_weight.shape[1] // LANE
    pairs = blocks // Z // 2
    singles = blocks // Z % 2 + (1 if blocks % Z else 0)
    chunks = pairs + singles
    bf, f32 = jnp.bfloat16, jnp.float32
    vm = pl.BlockSpec(memory_space=pltpu.VMEM)
    hbm = pl.BlockSpec(memory_space=pl.ANY)
    dma = pltpu.SemaphoreType.DMA

    def kernel(*refs):
        whole_kernel(Z, R, blocks, pairs, singles, refs)

    return pl.pallas_call(
        kernel,
        out_shape=pltpu.VMEM((T, D), bf),
        in_specs=[hbm] * 8 + [pl.BlockSpec(memory_space=pltpu.SMEM), vm, vm],
        out_specs=vm,
        scratch_shapes=[
            pltpu.VMEM((Z, T, VD), bf),
            pltpu.VMEM((S, T, 2 * VD), bf),
            pltpu.VMEM((pairs, S, W, 6 * LANE), bf),
            pltpu.VMEM((singles, S, W, 3 * LANE), bf),
            pltpu.VMEM((T, D), bf),
            pltpu.VMEM(out_weight.shape, bf),
            pltpu.VMEM((Z, T, VD), bf),
            pltpu.VMEM((Z, T, VD), bf),
            pltpu.VMEM((2, H, D), bf),
            pltpu.VMEM((H, D), bf),
            pltpu.VMEM((H, D), f32),
            pltpu.VMEM((H, D), bf),
            pltpu.VMEM((Z, 2, H, D), bf),
            pltpu.VMEM((T, (2 * pairs + singles) * LANE), bf),
            pltpu.VMEM((Z, T, D), f32),
            pltpu.VMEM((Z, H, D), bf),
            pltpu.VMEM((Z, H, D), bf),
            pltpu.VMEM((2, Z - 1, H, D), bf),
            pltpu.VMEM((2, Z - 1, H, D), bf),
            pltpu.VMEM((H, D), bf),
            dma((chunks + 1 + Z,)),
            dma((chunks + 2, Z - 1)),
            dma((chunks + 1,)),
            dma((chunks + 1, Z)),
            dma((chunks + 1,)),
            dma((chunks + 4,)),
            dma((Z + 1,)),
            dma((2,)),
            dma((2, Z)),
            dma((2, Z, SUB)),
            dma((2 * Z + 1,)),
            dma((Z + 1,)),
            dma((2, Z - 1)),
            dma((2, Z - 1, FINE)),
            dma((2,)),
        ],
        compiler_params=pltpu.CompilerParams(
            collective_id=0, has_side_effects=True, vmem_limit_bytes=VMEM_LIMIT
        ),
    )(
        queries,
        keys,
        values,
        gate_weight,
        up_weight,
        down_weight,
        resid,
        out_weight,
        lambdas,
        head_gain.reshape(1, -1),
        norm_gain.reshape(1, -1),
    )


def solution(mesh):
    sp, tp = mesh.shape["sp"], mesh.shape["tp"]

    def local(*args):
        heads = args[4].shape[0]
        tok_rows = args[1].shape[0]
        columns = (
            tp == 2
            and heads == 4
            and sp == 4 * heads
            and args[10].shape[1] == LANE
            and args[8].shape[0] == LANE
            and args[8].shape[1] % LANE == 0
            and args[8].shape[1] // LANE // heads == 5
            and args[8].shape[1] // LANE % heads == 2
            and tok_rows % (32 * FINE) == 0
            and FINE % SUB == 0
        )
        return (columns_form if columns else generic)(*args)

    return jax.shard_map(
        local,
        mesh=mesh,
        in_specs=(
            P("sp", None),
            P("sp", "tp"),
            P("sp", "tp"),
            P("sp", "tp"),
            P("tp"),
            P(),
            P("tp", None),
            P(),
            P("sp", "tp"),
            P("sp", "tp"),
            P("tp", "sp"),
        ),
        out_specs=P("sp", None),
        check_vma=False,
    )
```
